512 devices in a mesh: sp: 128 (over z, y, core), tp: 4 (over x).
Axes of the slice: x: 4, y: 8, z: 8, core: 2. Of those that a mesh axis runs over, the one named last changes fastest.
Arguments:
- tokens: bfloat16 [32768, 2048], P(('sp', 'tp')), may hold values from -6 to 6
- pre_gain: float32 [2048], replicated, may hold values from 0.1 to 1.9
- w_query_ret: bfloat16 [2048, 768], P('sp', 'tp'), may hold values from -0.125 to 0.125
- w_key_ret: bfloat16 [2048, 768], P('sp', 'tp'), may hold values from -0.125 to 0.125
- w_value_ret: bfloat16 [2048, 768], P('sp', 'tp'), may hold values from -0.125 to 0.125
- w_query_att: bfloat16 [2048, 768], P('sp', 'tp'), may hold values from -0.5 to 0.5
- w_key_att: bfloat16 [2048, 256], P('sp', 'tp'), may hold values from -0.125 to 0.125
- w_value_att: bfloat16 [2048, 256], P('sp', 'tp'), may hold values from -0.125 to 0.125
- w_out_ret: bfloat16 [768, 2048], P('tp', 'sp'), may hold values from -0.15625 to 0.15625
- w_out_att: bfloat16 [768, 2048], P('tp', 'sp'), may hold values from -0.15625 to 0.15625
- retain_log: float32 [32768, 12], P('sp', 'tp')
- forget_total: float32 [12, 32768], P('tp'), as said below
Outputs:
- mixed: bfloat16 [32768, 2048], P(('sp', 'tp'))
The draws below stay inside these ranges and needn't reach their ends.
Inputs may be any that keep to these rules, and one draw needn't show every extreme that they name: `forget_total`: never rises along positions.
All inputs are finite; a program needn't handle non-finite values.
Results may differ from the reference program's by a relative error of at most 0.019.
Values may be sent and summed in bfloat16 or wider, within the bound.
A program may use at most 64 MiB of HBM per device.

```python
import math
import jax
import jax.numpy as jnp
from jax import lax

D = 2048
HEAD = 64
R_HEADS = 12
F_HEADS = 12
KV_HEADS = 4
SPAN = 256
TOK_DEV = 256
TOKENS = 32768
N_TP = 4


def log_rates(key, heads):
    keys = jax.random.split(key, 6)
    order = jax.random.permutation(keys[0], heads)
    slow = order < heads // 2
    blocks = TOKENS // TOK_DEV
    spread = jnp.exp(jax.random.uniform(keys[1], (blocks, heads), jnp.float32, math.log(0.4), math.log(2.5)))
    spread = jnp.repeat(spread, TOK_DEV, axis=0)
    rough = jax.random.uniform(keys[2], (TOKENS, heads), jnp.float32, 0.5, 1.5)
    fast = jnp.exp(jax.random.uniform(keys[3], (heads,), jnp.float32, math.log(0.03), math.log(0.1)))
    base = jnp.where(slow, 0.2 * math.log(10.0) / TOKENS, fast)
    rates = base[None, :] * spread * rough
    places = jax.random.randint(keys[4], (2, heads), 0, TOKENS)
    losses = jax.random.uniform(keys[5], (2, heads), jnp.float32, 0.2, 0.4)
    struck = jnp.arange(TOKENS, dtype=jnp.int32)[:, None, None] == places[None, :, :]
    rates = rates - jnp.sum(jnp.where(struck, jnp.log(1.0 - losses)[None, :, :], 0.0), axis=1)
    return -rates


def draw_retain_log(key, part):
    return log_rates(jax.random.fold_in(key, 11), R_HEADS)


def draw_forget_total(key, part):
    return jnp.transpose(jnp.cumsum(log_rates(jax.random.fold_in(key, 23), F_HEADS), axis=0))


def block_levels(own_key, extent, cuts, least, high):
    factor_of, own = 1.0, jax.random.fold_in(own_key, 6)
    for dim, shards_of in cuts:
        heights = jnp.exp(jax.random.uniform(jax.random.fold_in(own, dim), (shards_of,), jnp.float32, least / len(cuts), high / len(cuts)))
        factor_of = factor_of * jnp.repeat(heights, extent[dim] // shards_of).reshape([-1 if axis == dim else 1 for axis in range(len(extent))])
    return factor_of


def scatter_about(stream_key, dims, deviation, reach, cuts=(), kind=jnp.bfloat16):
    values = deviation * jax.random.normal(stream_key, dims, jnp.float32)
    if cuts:
        values = values * block_levels(stream_key, dims, cuts, -0.22, 0.18)
    return jnp.clip(values, -reach, reach).astype(kind)


def setup_inputs(seed: int = 0) -> dict:
    seeds = jax.random.split(jax.random.key(seed), 13)
    tokens = scatter_about(seeds[0], (TOKENS, D), 1.0, 6.0, ((0, 512),))
    pre_gain = jnp.clip(1.0 + 0.18 * jax.random.normal(seeds[1], (D,), jnp.float32), 0.1, 1.9)
    w_query_ret = scatter_about(seeds[2], (D, R_HEADS * HEAD), D ** -0.5, 0.125, ((0, 128), (1, 4)))
    w_key_ret = scatter_about(seeds[3], (D, R_HEADS * HEAD), D ** -0.5, 0.125, ((0, 128), (1, 4)))
    w_value_ret = scatter_about(seeds[4], (D, R_HEADS * HEAD), D ** -0.5, 0.125, ((0, 128), (1, 4)))
    w_query_att = scatter_about(seeds[5], (D, F_HEADS * HEAD), (D // 16) ** -0.5, 0.5, ((0, 128), (1, 4)))
    w_key_att = scatter_about(seeds[6], (D, KV_HEADS * HEAD), D ** -0.5, 0.125, ((0, 128), (1, 4)))
    w_value_att = scatter_about(seeds[7], (D, KV_HEADS * HEAD), D ** -0.5, 0.125, ((0, 128), (1, 4)))
    w_out_ret = scatter_about(seeds[8], (R_HEADS * HEAD, D), (2 * R_HEADS * HEAD) ** -0.5, 0.15625, ((0, 4), (1, 128)))
    w_out_att = scatter_about(seeds[9], (F_HEADS * HEAD, D), (2 * F_HEADS * HEAD) ** -0.5, 0.15625, ((0, 4), (1, 128)))
    retain_log = draw_retain_log(jax.random.fold_in(seeds[12], 71), 0)
    forget_total = draw_forget_total(jax.random.fold_in(seeds[12], 71), 0)
    return dict(tokens=tokens, pre_gain=pre_gain, w_query_ret=w_query_ret, w_key_ret=w_key_ret, w_value_ret=w_value_ret, w_query_att=w_query_att, w_key_att=w_key_att, w_value_att=w_value_att, w_out_ret=w_out_ret, w_out_att=w_out_att, retain_log=retain_log, forget_total=forget_total)


EPS = 1e-06
THETA = 10000.0

def rotate(field, positions):
    half = field.shape[-1] // 2
    inverse = THETA ** (-jnp.arange(half, dtype=jnp.float32) / half)
    angles = positions[:, None] * inverse[None, :]
    cosine = jnp.cos(angles)[:, None, :]
    sine = jnp.sin(angles)[:, None, :]
    first_half = field[..., :half]
    second_half = field[..., half:]
    return jnp.concatenate([first_half * cosine - second_half * sine, first_half * sine + second_half * cosine], axis=-1)

def head_norm(values):
    centre = lax.optimization_barrier(jnp.mean(values, axis=-1, keepdims=True))
    spread = lax.optimization_barrier(jnp.mean(jnp.square(values - centre), axis=-1, keepdims=True))
    return (values - centre) * lax.rsqrt(spread + EPS)

def lowered(values):
    return lax.optimization_barrier(values.astype(jnp.bfloat16)).astype(jnp.float32)

def retain_block(state, inputs):
    query, key_rows, value_rows, logs = inputs
    within = jnp.cumsum(logs, axis=0)
    span = logs.shape[0]
    causal = jnp.arange(span)[:, None] >= jnp.arange(span)[None, :]
    scores = jnp.einsum('thd,shd->hts', query.astype(jnp.float32), key_rows.astype(jnp.float32))
    gap = jnp.where(causal, jnp.transpose(within)[:, :, None] - jnp.transpose(within)[:, None, :], 0.0)
    weights = jnp.where(causal, scores * jnp.exp(gap), 0.0).astype(jnp.bfloat16)
    local = jnp.einsum('hts,shd->thd', weights.astype(jnp.float32), value_rows.astype(jnp.float32))
    lifted = lowered(query.astype(jnp.float32) * jnp.exp(within)[:, :, None])
    carried = jnp.einsum('thd,hde->the', lifted, lowered(state))
    last = within[-1]
    faded = lowered(key_rows.astype(jnp.float32) * jnp.exp(last[None, :] - within)[:, :, None])
    update = jnp.einsum('shd,she->hde', faded, value_rows.astype(jnp.float32))
    return (jnp.exp(last)[:, None, None] * state + update, local + carried)

def project(normed, weight):
    return jnp.dot(normed, weight, preferred_element_type=jnp.float32)

def reference(tokens, pre_gain, w_query_ret, w_key_ret, w_value_ret, w_query_att, w_key_att, w_value_att, w_out_ret, w_out_att, retain_log, forget_total):
    rows = tokens.astype(jnp.float32)
    normed = (rows * lax.rsqrt(lax.optimization_barrier(jnp.mean(rows * rows, axis=-1, keepdims=True)) + EPS) * pre_gain.astype(jnp.float32)).astype(jnp.bfloat16)
    positions = jnp.arange(TOKENS, dtype=jnp.int32).astype(jnp.float32)
    shape = (TOKENS, R_HEADS, HEAD)
    ret_query = (rotate(project(normed, w_query_ret).reshape(shape), positions) * HEAD ** (-0.5)).astype(jnp.bfloat16)
    ret_key = rotate(project(normed, w_key_ret).reshape(shape), positions).astype(jnp.bfloat16)
    ret_value = project(normed, w_value_ret).astype(jnp.bfloat16).reshape(shape)
    blocks = TOKENS // SPAN
    start_state = jnp.zeros((R_HEADS, HEAD, HEAD), jnp.float32)
    inputs = (ret_query.reshape(blocks, SPAN, R_HEADS, HEAD), ret_key.reshape(blocks, SPAN, R_HEADS, HEAD), ret_value.reshape(blocks, SPAN, R_HEADS, HEAD), retain_log.reshape(blocks, SPAN, R_HEADS))
    _, inside = lax.scan(retain_block, start_state, inputs)
    retained = head_norm(inside.reshape(shape)).astype(jnp.bfloat16).reshape(TOKENS, R_HEADS * HEAD)
    group = F_HEADS // KV_HEADS
    pieces = TOKENS // TOK_DEV
    att_query = (project(normed, w_query_att) * HEAD ** (-0.5)).astype(jnp.bfloat16).reshape(pieces, TOK_DEV, KV_HEADS, group, HEAD)
    att_key = project(normed, w_key_att).astype(jnp.bfloat16).reshape(pieces, TOK_DEV, KV_HEADS, HEAD)
    att_value = project(normed, w_value_att).astype(jnp.bfloat16).reshape(pieces, TOK_DEV, KV_HEADS, HEAD)
    gates = forget_total.reshape(KV_HEADS, group, pieces, TOK_DEV)
    local_places = jnp.arange(TOK_DEV, dtype=jnp.int32)

    def attend_block(index):
        query_rows = lax.dynamic_index_in_dim(att_query, index, 0, keepdims=False).astype(jnp.float32)
        gate_rows = lax.dynamic_index_in_dim(gates, index, 2, keepdims=False)
        query_places = index * TOK_DEV + local_places

        def add_keys(other, carry):
            weighted, total = carry
            key_rows = lax.dynamic_index_in_dim(att_key, other, 0, keepdims=False).astype(jnp.float32)
            value_rows = lax.dynamic_index_in_dim(att_value, other, 0, keepdims=False).astype(jnp.float32)
            gate_keys = lax.dynamic_index_in_dim(gates, other, 2, keepdims=False)
            scores = jnp.einsum('tcgd,scd->cgts', query_rows, key_rows)
            logits = scores + gate_rows[:, :, :, None] - gate_keys[:, :, None, :]
            allowed = (other * TOK_DEV + local_places)[None, :] <= query_places[:, None]
            weights = jnp.exp(jnp.where(allowed, logits, -jnp.inf))
            total = total + lax.optimization_barrier(jnp.sum(weights, axis=-1))
            weighted = weighted + jnp.einsum('cgts,scd->cgtd', weights.astype(jnp.bfloat16).astype(jnp.float32), value_rows)
            return (weighted, total)
        init = (jnp.zeros((KV_HEADS, group, TOK_DEV, HEAD), jnp.float32), jnp.zeros((KV_HEADS, group, TOK_DEV), jnp.float32))
        weighted, total = lax.fori_loop(0, index + 1, add_keys, init)
        return (weighted / total[..., None]).astype(jnp.bfloat16)
    outputs = lax.map(attend_block, jnp.arange(pieces, dtype=jnp.int32))
    attended = jnp.transpose(outputs, (0, 3, 1, 2, 4)).reshape(TOKENS, F_HEADS * HEAD)
    ret_width = R_HEADS // N_TP * HEAD
    att_width = F_HEADS // N_TP * HEAD
    summed = jnp.zeros((TOKENS, D), jnp.float32)
    for part in range(N_TP):
        term = jnp.dot(retained[:, part * ret_width:(part + 1) * ret_width], w_out_ret[part * ret_width:(part + 1) * ret_width], preferred_element_type=jnp.float32)
        term = term + jnp.dot(attended[:, part * att_width:(part + 1) * att_width], w_out_att[part * att_width:(part + 1) * att_width], preferred_element_type=jnp.float32)
        summed = summed + lax.optimization_barrier(term.astype(jnp.bfloat16)).astype(jnp.float32)
    return summed.astype(jnp.bfloat16)
```

```python
import functools

import jax
import jax.numpy as jnp
from jax import lax
from jax.experimental import pallas as pl
from jax.experimental.pallas import tpu as pltpu
from jax.sharding import Mesh
from jax.sharding import PartitionSpec as P

HEAD = 64
SPAN = 256
SP = ("sp_0", "sp_1", "sp_2")
SP_TP = ("sp_0", "sp_1", "sp_2", "tp")
LOG2E = 1.4426950408889634
BY_NAME = pl.DeviceIdType.MESH

EPS = 1e-06
THETA = 10000.0

DELTAS = (0, 1, -1, 2, -2, 3, -3, 4)


def ring_plan():
    slots, count = {}, 0
    for j in range(1, 8):
        slots["first", j] = count
        count += 1
    for j in range(8):
        right = 4 if j % 2 == 0 else 3
        for step in range(right):
            slots["right", j, step] = count
            count += 1
        for step in range(7 - right):
            slots["left", j, step] = count
            count += 1
    return slots, count


SLOTS, N_SLOTS = ring_plan()
SUB_OF = {delta: j for j, delta in enumerate(DELTAS)}


class SpGather:
    def __init__(self, piece, bytes_of, send_sem, recv_sem, swap_send, swap_recv):
        self.piece, self.bytes_of = piece, bytes_of
        self.send_sem, self.recv_sem = send_sem, recv_sem
        self.swap_send, self.swap_recv = swap_send, swap_recv
        self.z, self.y, self.c = (lax.axis_index(a) for a in SP)

    def block(self, half, first, second):
        z, y = (second, first) if half == 0 else (first, second)
        return z * 16 + y * 2 + self.c

    def coords(self, half):
        return (self.y, self.z) if half == 0 else (self.z, self.y)

    def axes(self, half):
        return ("sp_1", "sp_0") if half == 0 else ("sp_0", "sp_1")

    def send(self, half, block, axis, by, slot):
        here = lax.axis_index(axis)
        ref = self.piece(half, block)
        pltpu.make_async_remote_copy(
            src_ref=ref,
            dst_ref=ref,
            send_sem=self.send_sem.at[half],
            recv_sem=self.recv_sem.at[half, slot],
            device_id={axis: lax.rem(here + by + 8, 8)},
            device_id_type=BY_NAME,
        ).start()

    def swap(self, half, block):
        ref = self.piece(half, block)
        pltpu.make_async_remote_copy(
            src_ref=ref,
            dst_ref=ref,
            send_sem=self.swap_send.at[half],
            recv_sem=self.swap_recv.at[half],
            device_id={"sp_2": 1 - self.c},
            device_id_type=BY_NAME,
        ).start()

    def arrived(self, half, block, slot):
        ref = self.piece(half, block)
        pltpu.make_async_copy(ref, ref, self.recv_sem.at[half, slot]).wait()

    def greet(self):
        barrier = pltpu.get_barrier_semaphore()
        for axis in ("sp_0", "sp_1"):
            for by in (1, 7):
                pl.semaphore_signal(
                    barrier,
                    inc=1,
                    device_id={axis: lax.rem(lax.axis_index(axis) + by, 8)},
                    device_id_type=BY_NAME,
                )
        pl.semaphore_signal(
            barrier, inc=1, device_id={"sp_2": 1 - self.c}, device_id_type=BY_NAME
        )
        pl.semaphore_wait(barrier, 5)

    def round(self, r):
        for half in (0, 1):
            a, b = self.coords(half)
            first, second = self.axes(half)
            if r == 0:
                own = self.block(half, a, b)
                self.send(half, own, first, 1, SLOTS["first", SUB_OF[1]])
                self.send(half, own, first, -1, SLOTS["first", SUB_OF[-1]])
            for delta in (r, -r) if 1 <= r <= 4 else ():
                if delta not in SUB_OF:
                    continue
                block = self.block(half, lax.rem(a - delta + 8, 8), b)
                self.arrived(half, block, SLOTS["first", SUB_OF[delta]])
                step = 1 if delta > 0 else -1
                if delta + step in SUB_OF:
                    self.send(half, block, first, step, SLOTS["first", SUB_OF[delta + step]])
            if r < 8:
                block = self.block(half, lax.rem(a - DELTAS[r] + 8, 8), b)
                self.send(half, block, second, 1, SLOTS["right", r, 0])
                self.send(half, block, second, -1, SLOTS["left", r, 0])
                self.swap(half, block)
            for step in range(4):
                j = r - 1 - step
                if not 0 <= j < 8:
                    continue
                source = lax.rem(a - DELTAS[j] + 8, 8)
                for way, by in (("right", 1), ("left", -1)):
                    if (way, j, step) not in SLOTS:
                        continue
                    block = self.block(half, source, lax.rem(b - by * (step + 1) + 8, 8))
                    self.arrived(half, block, SLOTS[way, j, step])
                    if (way, j, step + 1) in SLOTS:
                        self.send(half, block, second, by, SLOTS[way, j, step + 1])
                    self.swap(half, block)

    def finish(self):
        for half in (0, 1):
            swapped, sent = self.bytes_of(half, 64), self.bytes_of(half, 63)
            pltpu.make_async_copy(swapped, swapped, self.swap_recv.at[half]).wait()
            pltpu.make_async_copy(swapped, swapped, self.swap_send.at[half]).wait()
            pltpu.make_async_copy(sent, sent, self.send_sem.at[half]).wait()


GATHER_SEMS = [
    pltpu.SemaphoreType.DMA((2,)),
    pltpu.SemaphoreType.DMA((2, N_SLOTS)),
    pltpu.SemaphoreType.DMA((2,)),
    pltpu.SemaphoreType.DMA((2,)),
    pltpu.SemaphoreType.DMA,
]
ROUNDS = 12


def gather_kernel(shard_ref, out_ref, send_sem, recv_sem, swap_send, swap_recv, local_sem):
    rows, cols = shard_ref.shape
    if rows > cols:
        piece = lambda half, b: out_ref.at[b, pl.ds(half * (rows // 2), rows // 2)]
        many = lambda half, n: out_ref.at[pl.ds(0, n), pl.ds(half * (rows // 2), rows // 2)]
    else:
        piece = lambda half, b: out_ref.at[b, :, pl.ds(half * (cols // 2), cols // 2)]
        many = lambda half, n: out_ref.at[pl.ds(0, n), :, pl.ds(half * (cols // 2), cols // 2)]
    ring = SpGather(piece, many, send_sem, recv_sem, swap_send, swap_recv)
    own = ring.z * 16 + ring.y * 2 + ring.c
    copy = pltpu.make_async_copy(shard_ref, out_ref.at[own], local_sem)
    copy.start()
    ring.greet()
    copy.wait()
    for r in range(ROUNDS):
        ring.round(r)
    ring.finish()


def sp_gather(shard, collective_id):
    rows, cols = shard.shape
    return pl.pallas_call(
        gather_kernel,
        out_shape=jax.ShapeDtypeStruct((128, rows, cols), shard.dtype),
        in_specs=[pl.BlockSpec(memory_space=pltpu.VMEM)],
        out_specs=pl.BlockSpec(memory_space=pltpu.VMEM),
        scratch_shapes=GATHER_SEMS,
        compiler_params=pltpu.CompilerParams(
            collective_id=collective_id, has_side_effects=True, vmem_limit_bytes=40 * 2**20
        ),
    )(shard).reshape(128 * rows, cols)


def attend_kernel(q_ref, gate_rows_ref, gate_keys_ref, kv_ref, out_ref, acc, tot):
    z, y, c = (lax.axis_index(a) for a in SP)
    mine = z * 16 + y * 2 + c
    acc[...] = jnp.zeros_like(acc)
    tot[...] = jnp.zeros_like(tot)

    def weigh(block, masked):
        keys = kv_ref[pl.ds(pl.multiple_of(block * SPAN, SPAN), SPAN), :]
        for h in range(3):
            rows = pl.ds(h * SPAN, SPAN)
            scores = lax.dot_general(
                q_ref[rows, :], keys, (((1,), (1,)), ((), ())), preferred_element_type=jnp.float32
            )
            fall = gate_keys_ref[pl.ds(block, 1), h, :]
            logits = scores + (gate_rows_ref[rows, :] - fall)
            if masked:
                t = lax.broadcasted_iota(jnp.int32, logits.shape, 0)
                s = lax.broadcasted_iota(jnp.int32, logits.shape, 1)
                logits = jnp.where(s <= t, logits, -jnp.inf)
            weights = jnp.exp2(logits)
            tot[rows, :] += weights[:, :128] + weights[:, 128:]
            acc[rows, :] += jnp.dot(
                weights.astype(jnp.bfloat16), keys, preferred_element_type=jnp.float32
            )

    def pair(i, carry):
        weigh(2 * i, False)
        weigh(2 * i + 1, False)
        return carry

    lax.fori_loop(0, mine // 2, pair, 0)

    @pl.when(lax.rem(mine, 2) == 1)
    def _():
        weigh(mine - 1, False)

    weigh(mine, True)
    for h in range(3):
        rows = pl.ds(h * SPAN, SPAN)
        total = jnp.sum(tot[rows, :], axis=1, keepdims=True)
        out_ref[:, h * HEAD : (h + 1) * HEAD] = (acc[rows, HEAD:] / total).astype(jnp.bfloat16)


def attend(q, gate_rows, gate_keys, kv):
    return pl.pallas_call(
        attend_kernel,
        out_shape=jax.ShapeDtypeStruct((SPAN, 3 * HEAD), jnp.bfloat16),
        in_specs=[pl.BlockSpec(memory_space=pltpu.VMEM)] * 4,
        out_specs=pl.BlockSpec(memory_space=pltpu.VMEM),
        scratch_shapes=[
            pltpu.VMEM((3 * SPAN, 128), jnp.float32),
            pltpu.VMEM((3 * SPAN, 128), jnp.float32),
        ],
        compiler_params=pltpu.CompilerParams(vmem_limit_bytes=40 * 2**20),
    )(q, gate_rows, gate_keys, kv)


def from_everyone(shard, axis):
    copies = jnp.broadcast_to(shard, (lax.axis_size(axis), *shard.shape))
    return lax.all_to_all(copies, axis, split_axis=0, concat_axis=0, tiled=True)


def in_order(parts, dim):
    lengths = list(parts.shape[1:])
    lengths[dim] *= parts.shape[0]
    return jnp.moveaxis(parts, 0, dim).reshape(lengths)


def gathered_copies(shard, axis, dim):
    parts = from_everyone(shard, axis)
    return in_order(parts, dim)


def filled_with(shard, identity):
    return jax.tree.map(
        lambda part, zero: jnp.zeros_like(part) + jnp.asarray(zero, part.dtype), shard, identity
    )


def carried_in(shard, axes, combine, identity):
    before = start = filled_with(shard, identity)
    subtotal = shard
    for axis in reversed(axes):
        devices, here = (lax.axis_size(axis), lax.axis_index(axis))
        pieces = jax.tree.map(
            lambda part, kind: lax.all_gather(part.astype(kind), axis),
            subtotal,
            (jnp.bfloat16, jnp.bfloat16),
        )
        inside, subtotal = (start, start)
        for k in range(devices):
            passed = k < here
            subtotal = combine(
                subtotal, jax.tree.map(lambda part, own: part[k].astype(own.dtype), pieces, shard)
            )
            inside = jax.tree.map(lambda new, old: jnp.where(passed, new, old), subtotal, inside)
        before = combine(inside, before)
    return before


def cut_along(shard, dim, devices):
    lengths = shard.shape
    parts = shard.reshape(*lengths[:dim], devices, lengths[dim] // devices, *lengths[dim + 1 :])
    return jnp.moveaxis(parts, dim, 0)


def sent_and_summed(shard, axis, dim):
    devices = lax.axis_size(axis)
    parts = lax.all_to_all(cut_along(shard, dim, devices), axis, 0, 0, tiled=True)
    return jnp.sum(parts.astype(jnp.float32), axis=0)


def rotate(field, positions):
    half = field.shape[-1] // 2
    inverse = THETA ** (-jnp.arange(half, dtype=jnp.float32) / half)
    angles = positions[:, None] * inverse[None, :]
    cosine = jnp.cos(angles)[:, None, :]
    sine = jnp.sin(angles)[:, None, :]
    first_half = field[..., :half]
    second_half = field[..., half:]
    return jnp.concatenate(
        [first_half * cosine - second_half * sine, first_half * sine + second_half * cosine],
        axis=-1,
    )


def head_norm(values):
    centre = jnp.mean(values, axis=-1, keepdims=True)
    spread = jnp.mean(jnp.square(values - centre), axis=-1, keepdims=True)
    return (values - centre) * lax.rsqrt(spread + EPS)


def advance(state, pair):
    decay, update = pair
    return (jnp.exp(decay)[:, None, None] * state + update, state)


def body(
    tokens,
    pre_gain,
    w_query_ret,
    w_key_ret,
    w_value_ret,
    w_query_att,
    w_key_att,
    w_value_att,
    w_out_ret,
    w_out_att,
    retain_log,
    forget_total,
):
    rows = tokens.astype(jnp.float32)
    normed = (
        rows * lax.rsqrt(jnp.mean(rows * rows, axis=-1, keepdims=True) + EPS) * pre_gain
    ).astype(jnp.bfloat16)
    gathered = gathered_copies(normed, "tp", 0)
    tok_dev = gathered.shape[0]
    offset = lax.axis_index(SP) * tok_dev
    query_places = offset + jnp.arange(tok_dev, dtype=jnp.int32)
    positions = query_places.astype(jnp.float32)

    def blocked(values):
        return values.reshape((tok_dev // SPAN, SPAN) + values.shape[1:])

    matrices = sp_gather(
        jnp.concatenate(
            (
                w_query_ret,
                w_key_ret,
                w_value_ret,
                w_query_att,
                w_key_att,
                w_value_att,
                w_out_ret.T,
                w_out_att.T,
            ),
            axis=1,
        ),
        1,
    )
    flat = jnp.dot(gathered, matrices[:, :896], preferred_element_type=jnp.float32)
    projected = tuple(
        flat[:, a:b] for a, b in ((0, 192), (192, 384), (384, 576), (576, 768), (768, 896))
    )
    heads = retain_log.shape[1]
    shape = (tok_dev, heads, HEAD)
    query = blocked(
        (rotate(projected[0].reshape(shape), positions) * HEAD ** (-0.5)).astype(jnp.bfloat16)
    )
    key_rows = blocked(rotate(projected[1].reshape(shape), positions).astype(jnp.bfloat16))
    value_rows = blocked(projected[2].astype(jnp.bfloat16).reshape(shape))
    within = jnp.cumsum(blocked(retain_log), axis=1)
    causal = jnp.arange(SPAN)[:, None] >= jnp.arange(SPAN)[None, :]
    scores = jnp.einsum("bthd,bshd->bhts", query, key_rows, preferred_element_type=jnp.float32)
    turned = jnp.transpose(within, (0, 2, 1))
    gap = jnp.where(causal, turned[:, :, :, None] - turned[:, :, None, :], 0.0)
    weights = jnp.where(causal, scores * jnp.exp(gap), 0.0).astype(jnp.bfloat16)
    local = jnp.einsum("bhts,bshd->bthd", weights, value_rows, preferred_element_type=jnp.float32)
    last = within[:, -1]
    faded = (key_rows.astype(jnp.float32) * jnp.exp(last[:, None, :] - within)[..., None]).astype(
        jnp.bfloat16
    )
    updates = jnp.einsum("bshd,bshe->bhde", faded, value_rows, preferred_element_type=jnp.float32)
    zero_state = jnp.zeros((heads, HEAD, HEAD), jnp.float32)
    final, _ = lax.scan(advance, zero_state, (last, updates))
    decay_total = jnp.sum(last, axis=0)
    own_state = final.reshape(heads, HEAD * HEAD)

    def combine(earlier, later):
        return (earlier[0] + later[0], jnp.exp(later[0])[:, None] * earlier[1] + later[1])

    identity = (jnp.zeros_like(decay_total), jnp.zeros_like(own_state))
    incoming = carried_in((decay_total, own_state), SP, combine, identity)[1]
    _, befores = lax.scan(advance, incoming.reshape(heads, HEAD, HEAD), (last, updates))
    lifted = (query.astype(jnp.float32) * jnp.exp(within)[..., None]).astype(jnp.bfloat16)
    carried = jnp.einsum(
        "bthd,bhde->bthe", lifted, befores.astype(jnp.bfloat16), preferred_element_type=jnp.float32
    )
    retained = (
        head_norm((local + carried).reshape(shape))
        .astype(jnp.bfloat16)
        .reshape(tok_dev, heads * HEAD)
    )
    kv = sp_gather(projected[4].astype(jnp.bfloat16), 2)
    query = (projected[3] * (HEAD ** (-0.5) * LOG2E)).astype(jnp.bfloat16)
    query = query.reshape(tok_dev, 3, HEAD).transpose(1, 0, 2).reshape(3 * tok_dev, HEAD)
    query = jnp.pad(query, ((0, 0), (0, HEAD)))
    gates = forget_total * LOG2E
    gate_rows = lax.dynamic_slice_in_dim(gates, offset, tok_dev, 1).reshape(3 * tok_dev, 1)
    gate_keys = gates.reshape(3, 128, SPAN).transpose(1, 0, 2)
    attended = attend(query, gate_rows, gate_keys, kv)
    wide = jnp.concatenate((retained, attended), axis=1)
    mixed = sent_and_summed(
        lax.dot_general(
            wide, matrices[:, 896:], (((1,), (1,)), ((), ())), preferred_element_type=jnp.float32
        ).astype(jnp.bfloat16),
        "tp",
        0,
    )
    return mixed.astype(jnp.bfloat16)


def solution(mesh):
    finer = Mesh(mesh.devices.reshape(8, 8, 2, mesh.shape["tp"]), ("sp_0", "sp_1", "sp_2", "tp"))
    placed = (
        P(SP_TP, None),
        P(),
        P(SP, "tp"),
        P(SP, "tp"),
        P(SP, "tp"),
        P(SP, "tp"),
        P(SP, "tp"),
        P(SP, "tp"),
        P("tp", SP),
        P("tp", SP),
        P(SP, "tp"),
        P("tp", None),
    )
    return jax.shard_map(
        body, mesh=finer, in_specs=placed, out_specs=P(SP_TP, None), check_vma=False
    )
```

```python
import jax
import jax.numpy as jnp
from jax import lax
from jax.experimental import pallas as pl
from jax.experimental.pallas import tpu as pltpu
from jax.sharding import Mesh
from jax.sharding import PartitionSpec as P

HEAD = 64
SPAN = 256
SP = ("sp_0", "sp_1", "sp_2")
SP_TP = ("sp_0", "sp_1", "sp_2", "tp")
LOG2E = 1.4426950408889634
BY_NAME = pl.DeviceIdType.MESH

EPS = 1e-06
THETA = 10000.0

DELTAS = (0, 1, -1, 2, -2, 3, -3, 4)


def ring_plan():
    slots, count = {}, 0
    for j in range(1, 8):
        slots["first", j] = count
        count += 1
    for j in range(8):
        right = 4 if j % 2 == 0 else 3
        for step in range(right):
            slots["right", j, step] = count
            count += 1
        for step in range(7 - right):
            slots["left", j, step] = count
            count += 1
    return slots, count


SLOTS, N_SLOTS = ring_plan()
SUB_OF = {delta: j for j, delta in enumerate(DELTAS)}


class SpGather:
    def __init__(self, piece, bytes_of, send_sem, recv_sem, swap_send, swap_recv):
        self.piece, self.bytes_of = piece, bytes_of
        self.send_sem, self.recv_sem = send_sem, recv_sem
        self.swap_send, self.swap_recv = swap_send, swap_recv
        self.z, self.y, self.c = (lax.axis_index(a) for a in SP)

    def block(self, half, first, second):
        z, y = (second, first) if half == 0 else (first, second)
        return z * 16 + y * 2 + self.c

    def coords(self, half):
        return (self.y, self.z) if half == 0 else (self.z, self.y)

    def axes(self, half):
        return ("sp_1", "sp_0") if half == 0 else ("sp_0", "sp_1")

    def send(self, half, block, axis, by, slot):
        here = lax.axis_index(axis)
        ref = self.piece(half, block)
        pltpu.make_async_remote_copy(
            src_ref=ref,
            dst_ref=ref,
            send_sem=self.send_sem.at[half],
            recv_sem=self.recv_sem.at[half, slot],
            device_id={axis: lax.rem(here + by + 8, 8)},
            device_id_type=BY_NAME,
        ).start()

    def swap(self, half, block):
        ref = self.piece(half, block)
        pltpu.make_async_remote_copy(
            src_ref=ref,
            dst_ref=ref,
            send_sem=self.swap_send.at[half],
            recv_sem=self.swap_recv.at[half],
            device_id={"sp_2": 1 - self.c},
            device_id_type=BY_NAME,
        ).start()

    def arrived(self, half, block, slot):
        ref = self.piece(half, block)
        pltpu.make_async_copy(ref, ref, self.recv_sem.at[half, slot]).wait()

    def round(self, r):
        for half in (0, 1):
            a, b = self.coords(half)
            first, second = self.axes(half)
            if r == 0:
                own = self.block(half, a, b)
                self.send(half, own, first, 1, SLOTS["first", SUB_OF[1]])
                self.send(half, own, first, -1, SLOTS["first", SUB_OF[-1]])
            for delta in (r, -r) if 1 <= r <= 4 else ():
                if delta not in SUB_OF:
                    continue
                block = self.block(half, lax.rem(a - delta + 8, 8), b)
                self.arrived(half, block, SLOTS["first", SUB_OF[delta]])
                step = 1 if delta > 0 else -1
                if delta + step in SUB_OF:
                    self.send(half, block, first, step, SLOTS["first", SUB_OF[delta + step]])
            if r < 8:
                block = self.block(half, lax.rem(a - DELTAS[r] + 8, 8), b)
                self.send(half, block, second, 1, SLOTS["right", r, 0])
                self.send(half, block, second, -1, SLOTS["left", r, 0])
                self.swap(half, block)
            for step in range(4):
                j = r - 2 - 2 * step
                if not 0 <= j < 8:
                    continue
                source = lax.rem(a - DELTAS[j] + 8, 8)
                for way, by in (("right", 1), ("left", -1)):
                    if (way, j, step) not in SLOTS:
                        continue
                    block = self.block(half, source, lax.rem(b - by * (step + 1) + 8, 8))
                    self.arrived(half, block, SLOTS[way, j, step])
                    if (way, j, step + 1) in SLOTS:
                        self.send(half, block, second, by, SLOTS[way, j, step + 1])
                    self.swap(half, block)

    def finish(self):
        for half in (0, 1):
            swapped, sent = self.bytes_of(half, 64), self.bytes_of(half, 63)
            pltpu.make_async_copy(swapped, swapped, self.swap_recv.at[half]).wait()
            pltpu.make_async_copy(swapped, swapped, self.swap_send.at[half]).wait()
            pltpu.make_async_copy(sent, sent, self.send_sem.at[half]).wait()


def greet(*axes):
    barrier = pltpu.get_barrier_semaphore()
    count = 0
    for axis in axes:
        size = lax.axis_size(axis)
        for by in (1, size - 1) if size > 2 else (1,):
            pl.semaphore_signal(
                barrier,
                inc=1,
                device_id={axis: lax.rem(lax.axis_index(axis) + by, size)},
                device_id_type=BY_NAME,
            )
            count += 1
    pl.semaphore_wait(barrier, count)


def remote(src, dst, send_sem, recv_sem, axis, by):
    size = lax.axis_size(axis)
    return pltpu.make_async_remote_copy(
        src_ref=src,
        dst_ref=dst,
        send_sem=send_sem,
        recv_sem=recv_sem,
        device_id={axis: lax.rem(lax.axis_index(axis) + by + size, size)},
        device_id_type=BY_NAME,
    )


def wait_for(ref, sem):
    pltpu.make_async_copy(ref, ref, sem).wait()


GATHER_SEMS = [
    pltpu.SemaphoreType.DMA((2,)),
    pltpu.SemaphoreType.DMA((2, N_SLOTS)),
    pltpu.SemaphoreType.DMA((2,)),
    pltpu.SemaphoreType.DMA((2,)),
]
ROUNDS = 16
VMEM = pl.BlockSpec(memory_space=pltpu.VMEM)
IN_WIDTH = 896
ALL_WIDTH = 1280
WIDE = 3 * HEAD


def running_totals(logs):
    t = lax.broadcasted_iota(jnp.int32, (SPAN, SPAN), 0)
    s = lax.broadcasted_iota(jnp.int32, (SPAN, SPAN), 1)
    below = jnp.where(s <= t, 1.0, 0.0).astype(jnp.float32)
    dims = (((0,), (1,)), ((), ()))
    columns = jnp.dot(
        below, logs, preferred_element_type=jnp.float32, precision=lax.Precision.HIGHEST
    )
    rows = lax.dot_general(
        logs, below, dims, preferred_element_type=jnp.float32, precision=lax.Precision.HIGHEST
    )
    return columns, rows


def per_head(columns):
    rows = columns.shape[0]
    return jnp.concatenate(
        [jnp.broadcast_to(columns[:, h : h + 1], (rows, HEAD)) for h in range(3)], axis=1
    )


def project_kernel(
    tokens_ref,
    gain_ref,
    wqr_ref,
    wkr_ref,
    wvr_ref,
    wqa_ref,
    wka_ref,
    wva_ref,
    wor_ref,
    woa_ref,
    cos_ref,
    sin_ref,
    logs_ref,
    wall_ref,
    qr_ref,
    kr_ref,
    vr_ref,
    qa_ref,
    kv_ref,
    update_ref,
    total_ref,
    x_ref,
    send_sem,
    recv_sem,
    swap_send,
    swap_recv,
    x_send,
    x_recv,
):
    half_width = ALL_WIDTH // 2
    ring = SpGather(
        lambda half, b: wall_ref.at[b, :, pl.ds(half * half_width, half_width)],
        lambda half, n: wall_ref.at[pl.ds(0, n), :, pl.ds(half * half_width, half_width)],
        send_sem,
        recv_sem,
        swap_send,
        swap_recv,
    )
    own = ring.z * 16 + ring.y * 2 + ring.c
    x = lax.axis_index("tp")
    at = 0
    for ref in (wqr_ref, wkr_ref, wvr_ref, wqa_ref, wka_ref, wva_ref):
        wall_ref[own, :, at : at + ref.shape[1]] = ref[...]
        at += ref.shape[1]
    for ref in (wor_ref, woa_ref):
        wall_ref[own, :, at : at + WIDE] = ref[...].astype(jnp.float32).T.astype(jnp.bfloat16)
        at += WIDE
    rows = tokens_ref[...].astype(jnp.float32)
    x_ref[x] = (
        rows * lax.rsqrt(jnp.mean(rows * rows, axis=-1, keepdims=True) + EPS) * gain_ref[...]
    ).astype(jnp.bfloat16)
    greet("sp_0", "sp_1", "sp_2", "tp")
    ring.round(0)

    def part(slot, k):
        return x_ref.at[lax.rem(slot + 4, 4), :, pl.ds(k * 1024, 1024)]

    def pass_on(slot, k, by, sem):
        remote(part(slot, k), part(slot, k), x_send, x_recv.at[sem], "tp", by).start()

    pass_on(x, 0, 1, 0)
    pass_on(x, 1, -1, 1)
    pass_on(x, 1, 1, 2)
    pass_on(x, 0, -1, 3)
    ring.round(1)
    columns, _ = running_totals(logs_ref[...])
    last = columns[SPAN - 1 : SPAN]
    fade = jnp.exp(per_head(last - columns))
    total_ref[...] = jnp.broadcast_to(per_head(last), (8, WIDE))
    ring.round(2)
    ring.round(3)
    wait_for(part(x - 1, 0), x_recv.at[0])
    pass_on(x - 1, 0, 1, 4)
    wait_for(part(x + 1, 1), x_recv.at[1])
    pass_on(x + 1, 1, -1, 5)
    for r in range(4, ROUNDS):
        ring.round(r)
    wait_for(part(x - 1, 1), x_recv.at[2])
    wait_for(part(x + 1, 0), x_recv.at[3])
    wait_for(part(x - 2, 0), x_recv.at[4])
    wait_for(part(x + 2, 1), x_recv.at[5])
    ring.finish()
    sent = x_ref.at[pl.ds(0, 3)]
    wait_for(sent, x_send)

    flat = jnp.dot(
        x_ref[...].reshape(SPAN, 2048),
        wall_ref[:, :, :IN_WIDTH].reshape(2048, IN_WIDTH),
        preferred_element_type=jnp.float32,
    )
    both = flat[:, : 2 * WIDE]
    lane = lax.rem(lax.broadcasted_iota(jnp.int32, both.shape, 1), HEAD)
    turned = jnp.where(
        lane < HEAD // 2, pltpu.roll(both, 2 * WIDE - HEAD // 2, 1), pltpu.roll(both, HEAD // 2, 1)
    )
    cosine = jnp.concatenate([cos_ref[...]] * 3, axis=1)
    sine = jnp.concatenate([sin_ref[...]] * 3, axis=1)
    roped = both * cosine + turned * sine
    qr_ref[...] = (roped[:, :WIDE] * HEAD**-0.5).astype(jnp.bfloat16)
    key = roped[:, WIDE:].astype(jnp.bfloat16)
    kr_ref[...] = key
    value = flat[:, 2 * WIDE : 3 * WIDE].astype(jnp.bfloat16)
    vr_ref[...] = value
    faded = (key.astype(jnp.float32) * fade).astype(jnp.bfloat16)
    for h in range(3):
        lanes = slice(h * HEAD, (h + 1) * HEAD)
        update_ref[:, lanes] = lax.dot_general(
            faded[:, lanes],
            value[:, lanes],
            (((0,), (0,)), ((), ())),
            preferred_element_type=jnp.float32,
        )
        query = flat[:, 3 * WIDE + h * HEAD : 3 * WIDE + (h + 1) * HEAD] * (HEAD**-0.5 * LOG2E)
        qa_ref[h * SPAN : (h + 1) * SPAN, :] = jnp.concatenate(
            [query, jnp.zeros_like(query)], axis=1
        ).astype(jnp.bfloat16)
    kv_ref[...] = flat[:, 4 * WIDE :].astype(jnp.bfloat16)


def project(*operands):
    bf16 = jnp.bfloat16
    square = jax.ShapeDtypeStruct((SPAN, WIDE), bf16)
    return pl.pallas_call(
        project_kernel,
        out_shape=(
            jax.ShapeDtypeStruct((128, 16, ALL_WIDTH), bf16),
            square,
            square,
            square,
            jax.ShapeDtypeStruct((3 * SPAN, 128), bf16),
            jax.ShapeDtypeStruct((SPAN, 128), bf16),
            jax.ShapeDtypeStruct((HEAD, WIDE), jnp.float32),
            jax.ShapeDtypeStruct((8, WIDE), jnp.float32),
        ),
        in_specs=[VMEM] * len(operands),
        out_specs=(VMEM,) * 8,
        scratch_shapes=[
            pltpu.VMEM((4, 64, 2048), bf16),
            *GATHER_SEMS,
            pltpu.SemaphoreType.DMA,
            pltpu.SemaphoreType.DMA((6,)),
        ],
        compiler_params=pltpu.CompilerParams(
            collective_id=1, has_side_effects=True, vmem_limit_bytes=40 * 2**20
        ),
    )(*operands)


class Prefix:
    def __init__(self, states, decays, sems):
        self.states, self.decays = states, decays
        self.state_send, self.state_recv, self.decay_send, self.decay_recv = sems
        self.z, self.y, self.c = (lax.axis_index(a) for a in SP)

    def send(self, slot, axis, by, sem):
        for ref, out, arrive in (
            (self.states, self.state_send, self.state_recv),
            (self.decays, self.decay_send, self.decay_recv),
        ):
            remote(ref.at[slot], ref.at[slot], out, arrive.at[sem], axis, by).start()

    def wait(self, slot, sem):
        wait_for(self.states.at[slot], self.state_recv.at[sem])
        wait_for(self.decays.at[slot], self.decay_recv.at[sem])

    def store(self, slot, pair):
        self.states[slot] = pair[0].astype(jnp.bfloat16)
        self.decays[slot] = pair[1]

    def load(self, slot):
        return self.states[slot].astype(jnp.float32), self.decays[slot]

    @staticmethod
    def join(earlier, later):
        return jnp.exp(later[1][:1]) * earlier[0] + later[0], earlier[1] + later[1]

    @staticmethod
    def keep(flag, pair):
        return jnp.where(flag, pair[0], 0.0), jnp.where(flag, pair[1], 0.0)

    def ring_hop(self, hop, base, here, axis, first_sem):
        if hop == 0:
            self.send(base + here, axis, 1, first_sem)
            self.send(base + here, axis, -1, first_sem + 4)
            return
        right = base + lax.rem(here - hop + 8, 8)
        self.wait(right, first_sem + hop - 1)
        if hop < 4:
            self.send(right, axis, 1, first_sem + hop)
            left = base + lax.rem(here + hop, 8)
            self.wait(left, first_sem + 4 + hop - 1)
            if hop < 3:
                self.send(left, axis, -1, first_sem + 4 + hop)

    def round(self, r):
        if r == 0:
            self.send(self.c, "sp_2", 1, 0)
        if r == 1:
            self.wait(1 - self.c, 0)
            self.store(2 + self.y, self.join(self.load(0), self.load(1)))
            self.ring_hop(0, 2, self.y, "sp_1", 1)
        if r in (3, 5, 7, 9):
            self.ring_hop((r - 1) // 2, 2, self.y, "sp_1", 1)
        if r == 9:
            total = self.load(2)
            for k in range(1, 8):
                total = self.join(total, self.load(2 + k))
            self.store(10 + self.z, total)
            self.ring_hop(0, 10, self.z, "sp_0", 8)
        if r in (11, 13, 15, 17):
            self.ring_hop((r - 9) // 2, 10, self.z, "sp_0", 8)

    def finish(self):
        before = self.keep(0 < self.z, self.load(10))
        for k in range(1, 7):
            before = self.keep_if(k < self.z, before, self.load(10 + k))
        for k in range(7):
            before = self.keep_if(k < self.y, before, self.load(2 + k))
        before = self.keep_if(self.c == 1, before, self.load(0))
        for ref, sem in ((self.states, self.state_send), (self.decays, self.decay_send)):
            wait_for(ref.at[pl.ds(0, 15)], sem)
        return before[0]

    def keep_if(self, flag, before, later):
        return self.join(before, self.keep(flag, later))


PREFIX_SEMS = [
    pltpu.SemaphoreType.DMA,
    pltpu.SemaphoreType.DMA((15,)),
    pltpu.SemaphoreType.DMA,
    pltpu.SemaphoreType.DMA((15,)),
]


def exchange_kernel(
    kv_ref,
    update_ref,
    total_ref,
    kvs_ref,
    before_ref,
    states,
    decays,
    local_sem,
    send_sem,
    recv_sem,
    swap_send,
    swap_recv,
    *prefix_sems,
):
    rows = SPAN // 2
    ring = SpGather(
        lambda half, b: kvs_ref.at[b, pl.ds(half * rows, rows)],
        lambda half, n: kvs_ref.at[pl.ds(0, n), pl.ds(half * rows, rows)],
        send_sem,
        recv_sem,
        swap_send,
        swap_recv,
    )
    prefix = Prefix(states, decays, prefix_sems)
    own = ring.z * 16 + ring.y * 2 + ring.c
    copy = pltpu.make_async_copy(kv_ref, kvs_ref.at[own], local_sem)
    copy.start()
    prefix.store(ring.c, (update_ref[...], total_ref[...]))
    greet(*SP)
    copy.wait()
    for r in range(18):
        prefix.round(r)
        if r < ROUNDS:
            ring.round(r)
    before_ref[...] = prefix.finish().astype(jnp.bfloat16)
    ring.finish()


def exchange(kv, update, total):
    return pl.pallas_call(
        exchange_kernel,
        out_shape=(
            jax.ShapeDtypeStruct((128, SPAN, 128), jnp.bfloat16),
            jax.ShapeDtypeStruct((HEAD, WIDE), jnp.bfloat16),
        ),
        in_specs=[VMEM] * 3,
        out_specs=(VMEM,) * 2,
        scratch_shapes=[
            pltpu.VMEM((18, HEAD, WIDE), jnp.bfloat16),
            pltpu.VMEM((18, 8, WIDE), jnp.float32),
            pltpu.SemaphoreType.DMA,
            *GATHER_SEMS,
            *PREFIX_SEMS,
        ],
        compiler_params=pltpu.CompilerParams(
            collective_id=2, has_side_effects=True, vmem_limit_bytes=40 * 2**20
        ),
    )(kv, update, total)


def retain(qr_ref, kr_ref, vr_ref, logs, before, out_ref):
    columns, rows = running_totals(logs)
    t = lax.broadcasted_iota(jnp.int32, (SPAN, SPAN), 0)
    s = lax.broadcasted_iota(jnp.int32, (SPAN, SPAN), 1)
    causal = s <= t
    lifted = (qr_ref[...].astype(jnp.float32) * jnp.exp(per_head(columns))).astype(jnp.bfloat16)
    for h in range(3):
        lanes = slice(h * HEAD, (h + 1) * HEAD)
        scores = lax.dot_general(
            qr_ref[:, lanes],
            kr_ref[:, lanes],
            (((1,), (1,)), ((), ())),
            preferred_element_type=jnp.float32,
        )
        gap = jnp.where(causal, columns[:, h : h + 1] - rows[h : h + 1, :], 0.0)
        weights = jnp.where(causal, scores * jnp.exp(gap), 0.0).astype(jnp.bfloat16)
        raw = jnp.dot(weights, vr_ref[:, lanes], preferred_element_type=jnp.float32)
        raw += jnp.dot(lifted[:, lanes], before[:, lanes], preferred_element_type=jnp.float32)
        raw -= jnp.mean(raw, axis=-1, keepdims=True)
        spread = jnp.mean(raw * raw, axis=-1, keepdims=True)
        out_ref[:, lanes] = (raw * lax.rsqrt(spread + EPS)).astype(jnp.bfloat16)


def mix_kernel(
    qr_ref, kr_ref, vr_ref, logs_ref, before_ref, qa_ref, gates_ref, kvs_ref, wall_ref,
    out_ref, acc, tot, wide
):
    z, y, c = (lax.axis_index(a) for a in SP)
    mine = z * 16 + y * 2 + c
    retain(qr_ref, kr_ref, vr_ref, logs_ref[...], before_ref[...], wide)
    acc[...] = jnp.zeros_like(acc)
    tot[...] = jnp.zeros_like(tot)

    def gate_row(block, h):
        span = pl.ds(pl.multiple_of(block * SPAN, SPAN), SPAN)
        return gates_ref[h : h + 1, span] * LOG2E

    gate_columns = jnp.transpose(
        jnp.concatenate(
            [gate_row(mine, h) for h in range(3)] + [jnp.zeros((5, SPAN), jnp.float32)], axis=0
        )
    )

    def weigh(block, masked):
        keys = kvs_ref[block]
        for h in range(3):
            rows = pl.ds(h * SPAN, SPAN)
            scores = lax.dot_general(
                qa_ref[rows, :], keys, (((1,), (1,)), ((), ())), preferred_element_type=jnp.float32
            )
            logits = scores + (gate_columns[:, h : h + 1] - gate_row(block, h))
            if masked:
                t = lax.broadcasted_iota(jnp.int32, logits.shape, 0)
                s = lax.broadcasted_iota(jnp.int32, logits.shape, 1)
                logits = jnp.where(s <= t, logits, -jnp.inf)
            weights = jnp.exp2(logits)
            tot[rows, :] += weights[:, :128] + weights[:, 128:]
            acc[rows, :] += jnp.dot(
                weights.astype(jnp.bfloat16), keys, preferred_element_type=jnp.float32
            )

    def pair(i, carry):
        weigh(2 * i, False)
        weigh(2 * i + 1, False)
        return carry

    lax.fori_loop(0, mine // 2, pair, 0)

    @pl.when(lax.rem(mine, 2) == 1)
    def _():
        weigh(mine - 1, False)

    weigh(mine, True)
    for h in range(3):
        rows = pl.ds(h * SPAN, SPAN)
        total = jnp.sum(tot[rows, :], axis=1, keepdims=True)
        wide[:, WIDE + h * HEAD : WIDE + (h + 1) * HEAD] = (acc[rows, HEAD:] / total).astype(
            jnp.bfloat16
        )
    for k in range(4):
        columns = wall_ref[k * 32 : (k + 1) * 32, :, IN_WIDTH:].reshape(512, 2 * WIDE)
        out_ref[:, k * 512 : (k + 1) * 512] = lax.dot_general(
            wide[...], columns, (((1,), (1,)), ((), ())), preferred_element_type=jnp.float32
        ).astype(jnp.bfloat16)


def mix(*operands):
    return pl.pallas_call(
        mix_kernel,
        out_shape=jax.ShapeDtypeStruct((SPAN, 2048), jnp.bfloat16),
        in_specs=[VMEM] * len(operands),
        out_specs=VMEM,
        scratch_shapes=[
            pltpu.VMEM((3 * SPAN, 128), jnp.float32),
            pltpu.VMEM((3 * SPAN, 128), jnp.float32),
            pltpu.VMEM((SPAN, 2 * WIDE), jnp.bfloat16),
        ],
        compiler_params=pltpu.CompilerParams(vmem_limit_bytes=40 * 2**20),
    )(*operands)


def cut_along(shard, dim, devices):
    lengths = shard.shape
    parts = shard.reshape(*lengths[:dim], devices, lengths[dim] // devices, *lengths[dim + 1 :])
    return jnp.moveaxis(parts, dim, 0)


def sent_and_summed(shard, axis, dim):
    devices = lax.axis_size(axis)
    parts = lax.all_to_all(cut_along(shard, dim, devices), axis, 0, 0, tiled=True)
    return jnp.sum(parts.astype(jnp.float32), axis=0)


def angles_of(positions):
    half = HEAD // 2
    inverse = THETA ** (-jnp.arange(half, dtype=jnp.float32) / half)
    return positions[:, None] * inverse[None, :]


def body(
    tokens,
    pre_gain,
    w_query_ret,
    w_key_ret,
    w_value_ret,
    w_query_att,
    w_key_att,
    w_value_att,
    w_out_ret,
    w_out_att,
    retain_log,
    forget_total,
):
    offset = lax.axis_index(SP) * SPAN
    positions = (offset + jnp.arange(SPAN, dtype=jnp.int32)).astype(jnp.float32)
    angles = angles_of(positions)
    cosine, sine = jnp.cos(angles), jnp.sin(angles)
    cosine = jnp.concatenate([cosine] * 4, axis=1)
    sine = jnp.concatenate([-sine, sine] * 2, axis=1)
    wall, qr, kr, vr, qa, kv, update, total = project(
        tokens,
        pre_gain.reshape(1, -1),
        w_query_ret,
        w_key_ret,
        w_value_ret,
        w_query_att,
        w_key_att,
        w_value_att,
        w_out_ret,
        w_out_att,
        cosine,
        sine,
        retain_log,
    )
    kvs, before = exchange(kv, update, total)
    partial = mix(qr, kr, vr, retain_log, before, qa, forget_total, kvs, wall)
    return sent_and_summed(partial, "tp", 0).astype(jnp.bfloat16)


def solution(mesh):
    finer = Mesh(mesh.devices.reshape(8, 8, 2, mesh.shape["tp"]), ("sp_0", "sp_1", "sp_2", "tp"))
    placed = (
        P(SP_TP, None),
        P(),
        P(SP, "tp"),
        P(SP, "tp"),
        P(SP, "tp"),
        P(SP, "tp"),
        P(SP, "tp"),
        P(SP, "tp"),
        P("tp", SP),
        P("tp", SP),
        P(SP, "tp"),
        P("tp", None),
    )
    return jax.shard_map(
        body, mesh=finer, in_specs=placed, out_specs=P(SP_TP, None), check_vma=False
    )
```

```python
import jax
import jax.numpy as jnp
from jax import lax
from jax.experimental import pallas as pl
from jax.experimental.pallas import tpu as pltpu
from jax.sharding import Mesh
from jax.sharding import PartitionSpec as P

HEAD = 64
SPAN = 256
SP = ("sp_0", "sp_1", "sp_2")
SP_TP = ("sp_0", "sp_1", "sp_2", "tp")
LOG2E = 1.4426950408889634
BY_NAME = pl.DeviceIdType.MESH
VMEM = pl.BlockSpec(memory_space=pltpu.VMEM)
ANY = pl.BlockSpec(memory_space=pl.ANY)
IN_WIDTH = 896
ALL_WIDTH = 1280
WIDE = 3 * HEAD

EPS = 1e-06
THETA = 10000.0

DELTAS = (0, 1, -1, 2, -2, 3, -3, 4)


def ring_plan():
    slots = {}
    for delta in DELTAS[1:]:
        slots["first", delta] = len(slots)
    for delta in DELTAS:
        right = 4 if delta <= 0 else 3
        for way, steps in ((1, right), (-1, 7 - right)):
            for step in range(steps):
                slots[way, delta, step] = len(slots)
    return slots


SLOTS = ring_plan()
STEPS = 9


def greet(*axes):
    barrier = pltpu.get_barrier_semaphore()
    count = 0
    for axis in axes:
        size = lax.axis_size(axis)
        for by in (1, size - 1) if size > 2 else (1,):
            pl.semaphore_signal(
                barrier,
                inc=1,
                device_id={axis: lax.rem(lax.axis_index(axis) + by, size)},
                device_id_type=BY_NAME,
            )
            count += 1
    return lambda: pl.semaphore_wait(barrier, count)


def remote(src, dst, send_sem, recv_sem, axis, by):
    size = lax.axis_size(axis)
    return pltpu.make_async_remote_copy(
        src_ref=src,
        dst_ref=dst,
        send_sem=send_sem,
        recv_sem=recv_sem,
        device_id={axis: lax.rem(lax.axis_index(axis) + by + size, size)},
        device_id_type=BY_NAME,
    )


def wait_for(ref, sem):
    pltpu.make_async_copy(ref, ref, sem).wait()


def ring_index(at):
    return lax.rem(at + 8, 8)


class SpGather:
    def __init__(self, ref, part, sems):
        self.ref, self.part = ref, part
        self.send_sem, self.recv_sem, self.swap_send, self.swap_recv = sems
        self.z, self.y, self.c = (lax.axis_index(a) for a in SP)

    def piece(self, half, first, second):
        z, y = (second, first) if half == 0 else (first, second)
        return self.ref.at[(z, y, self.c) + self.part(half)]

    def slab(self, half, second):
        place = (second, slice(None)) if half == 0 else (slice(None), second)
        return self.ref.at[place + (self.c,) + self.part(half)]

    def coords(self, half):
        return (self.y, self.z) if half == 0 else (self.z, self.y)

    def send(self, half, ref, axis, by, slot):
        remote(
            ref, ref, self.send_sem.at[half], self.recv_sem.at[half, SLOTS[slot]], axis, by
        ).start()

    def arrived(self, half, ref, slot):
        wait_for(ref, self.recv_sem.at[half, SLOTS[slot]])

    def swap(self, half, second):
        ref = self.slab(half, second)
        remote(ref, ref, self.swap_send.at[half], self.swap_recv.at[half], "sp_2", 1).start()

    def step(self, s):
        for half in (0, 1):
            a, b = self.coords(half)
            first, second = ("sp_1", "sp_0") if half == 0 else ("sp_0", "sp_1")
            for delta in sorted({s, -s}, reverse=True):
                if delta not in DELTAS:
                    continue
                ref = self.piece(half, ring_index(a - delta), b)
                if delta:
                    self.arrived(half, ref, ("first", delta))
                for further in (1, -1) if delta == 0 else (delta + (1 if delta > 0 else -1),):
                    if further in DELTAS:
                        self.send(half, ref, first, 1 if further > 0 else -1, ("first", further))
                for by in (1, -1):
                    self.send(half, ref, second, by, (by, delta, 0))
            if s == 4:
                self.swap(half, b)
            for k in range(4):
                for delta in DELTAS:
                    if abs(delta) != s - 1 - k:
                        continue
                    for by in (1, -1):
                        if (by, delta, k) not in SLOTS:
                            continue
                        ref = self.piece(half, ring_index(a - delta), ring_index(b - by * (k + 1)))
                        self.arrived(half, ref, (by, delta, k))
                        if (by, delta, k + 1) in SLOTS:
                            self.send(half, ref, second, by, (by, delta, k + 1))
            if 5 <= s < 8:
                self.swap(half, ring_index(b - (s - 4)))
                self.swap(half, ring_index(b + (s - 4)))
            if s == 8:
                self.swap(half, ring_index(b + 4))

    def finish(self):
        for half in (0, 1):
            core = self.ref.at[(slice(None), slice(None), 0) + self.part(half)]
            wait_for(core, self.swap_recv.at[half])
            wait_for(core, self.swap_send.at[half])
            wait_for(
                self.ref.at[(slice(0, 7), slice(None), 0) + self.part(half)],
                self.send_sem.at[half],
            )
            wait_for(
                self.ref.at[(0, slice(0, 7), 0) + self.part(half)], self.send_sem.at[half]
            )


GATHER_SEMS = [
    pltpu.SemaphoreType.DMA((2,)),
    pltpu.SemaphoreType.DMA((2, len(SLOTS))),
    pltpu.SemaphoreType.DMA((2,)),
    pltpu.SemaphoreType.DMA((2,)),
]


def running_totals(logs):
    t = lax.broadcasted_iota(jnp.int32, (SPAN, SPAN), 0)
    s = lax.broadcasted_iota(jnp.int32, (SPAN, SPAN), 1)
    below = jnp.where(s <= t, 1.0, 0.0).astype(jnp.float32)
    dims = (((1,), (1,)), ((), ()))
    exact = lax.Precision.HIGHEST
    columns = lax.dot_general(
        below, logs, dims, preferred_element_type=jnp.float32, precision=exact
    )
    rows = lax.dot_general(logs, below, dims, preferred_element_type=jnp.float32, precision=exact)
    return columns, rows


def per_head(columns):
    rows = columns.shape[0]
    return jnp.concatenate(
        [jnp.broadcast_to(columns[:, h : h + 1], (rows, HEAD)) for h in range(3)], axis=1
    )


class Prefix:
    def __init__(self, states, decays, sems):
        self.states, self.decays = states, decays
        self.state_send, self.state_recv, self.decay_send, self.decay_recv = sems
        self.z, self.y, self.c = (lax.axis_index(a) for a in SP)

    def send(self, slot, axis, by, sem):
        for ref, out, arrive in (
            (self.states, self.state_send, self.state_recv),
            (self.decays, self.decay_send, self.decay_recv),
        ):
            remote(ref.at[slot], ref.at[slot], out, arrive.at[sem], axis, by).start()

    def wait(self, slot, sem):
        wait_for(self.states.at[slot], self.state_recv.at[sem])
        wait_for(self.decays.at[slot], self.decay_recv.at[sem])

    def store(self, slot, pair):
        self.states[slot] = pair[0].astype(jnp.bfloat16)
        self.decays[slot] = pair[1]

    def load(self, slot):
        return self.states[slot].astype(jnp.float32), self.decays[slot]

    @staticmethod
    def join(earlier, later):
        return jnp.exp(later[1][:1]) * earlier[0] + later[0], earlier[1] + later[1]

    @staticmethod
    def keep(flag, pair):
        return jnp.where(flag, pair[0], 0.0), jnp.where(flag, pair[1], 0.0)

    def ring_hop(self, hop, base, here, axis, first_sem):
        if hop == 0:
            self.send(base + here, axis, 1, first_sem)
            self.send(base + here, axis, -1, first_sem + 4)
            return
        right = base + lax.rem(here - hop + 8, 8)
        self.wait(right, first_sem + hop - 1)
        if hop < 4:
            self.send(right, axis, 1, first_sem + hop)
            left = base + lax.rem(here + hop, 8)
            self.wait(left, first_sem + 4 + hop - 1)
            if hop < 3:
                self.send(left, axis, -1, first_sem + 4 + hop)

    def step(self, s):
        if s == 0:
            self.send(self.c, "sp_2", 1, 0)
        if s == 1:
            self.wait(1 - self.c, 0)
            self.store(2 + self.y, self.join(self.load(0), self.load(1)))
            self.ring_hop(0, 2, self.y, "sp_1", 1)
        if 2 <= s <= 5:
            self.ring_hop(s - 1, 2, self.y, "sp_1", 1)
        if s == 5:
            total = self.load(2)
            for k in range(1, 8):
                total = self.join(total, self.load(2 + k))
            self.store(10 + self.z, total)
            self.ring_hop(0, 10, self.z, "sp_0", 8)
        if 6 <= s <= 9:
            self.ring_hop(s - 5, 10, self.z, "sp_0", 8)

    def finish(self):
        before = self.keep(0 < self.z, self.load(10))
        for k in range(1, 7):
            before = self.keep_if(k < self.z, before, self.load(10 + k))
        for k in range(7):
            before = self.keep_if(k < self.y, before, self.load(2 + k))
        before = self.keep_if(self.c == 1, before, self.load(0))
        for ref, sem in ((self.states, self.state_send), (self.decays, self.decay_send)):
            wait_for(ref.at[pl.ds(0, 15)], sem)
        return before[0]

    def keep_if(self, flag, before, later):
        return self.join(before, self.keep(flag, later))


PREFIX_SEMS = [
    pltpu.SemaphoreType.DMA,
    pltpu.SemaphoreType.DMA((15,)),
    pltpu.SemaphoreType.DMA,
    pltpu.SemaphoreType.DMA((15,)),
]


def retain_inside(qr_ref, kr_ref, vr_ref, logs, raw_ref, lifted_ref):
    columns, rows = running_totals(logs)
    t = lax.broadcasted_iota(jnp.int32, (SPAN, SPAN), 0)
    s = lax.broadcasted_iota(jnp.int32, (SPAN, SPAN), 1)
    causal = s <= t
    lifted = qr_ref[...].astype(jnp.float32) * jnp.exp(per_head(columns))
    lifted_ref[...] = lifted.astype(jnp.bfloat16)
    for h in range(3):
        lanes = slice(h * HEAD, (h + 1) * HEAD)
        scores = lax.dot_general(
            qr_ref[:, lanes],
            kr_ref[:, lanes],
            (((1,), (1,)), ((), ())),
            preferred_element_type=jnp.float32,
        )
        gap = jnp.where(causal, columns[:, h : h + 1] - rows[h : h + 1, :], 0.0)
        weights = jnp.where(causal, scores * jnp.exp(gap), 0.0).astype(jnp.bfloat16)
        raw_ref[:, lanes] = jnp.dot(
            weights, vr_ref[:, lanes], preferred_element_type=jnp.float32
        )


def retain_earlier(raw_ref, lifted_ref, before, wide_ref):
    for h in range(3):
        lanes = slice(h * HEAD, (h + 1) * HEAD)
        raw = raw_ref[:, lanes] + jnp.dot(
            lifted_ref[:, lanes], before[:, lanes], preferred_element_type=jnp.float32
        )
        raw -= jnp.mean(raw, axis=-1, keepdims=True)
        spread = jnp.mean(raw * raw, axis=-1, keepdims=True)
        wide_ref[:, lanes] = (raw * lax.rsqrt(spread + EPS)).astype(jnp.bfloat16)


def layer_kernel(
    tokens_ref,
    gain_ref,
    wqr_ref,
    wkr_ref,
    wvr_ref,
    wqa_ref,
    wka_ref,
    wva_ref,
    wor_ref,
    woa_ref,
    cos_ref,
    sin_ref,
    logs_ref,
    gates_ref,
    out_ref,
    tokens_in,
    gain_in,
    wqr_in,
    wkr_in,
    wvr_in,
    wqa_in,
    wka_in,
    wva_in,
    wor_in,
    woa_in,
    cos_in,
    sin_in,
    logs_in,
    gates_in,
    wall_ref,
    x_ref,
    qr_ref,
    kr_ref,
    vr_ref,
    qa_ref,
    update,
    kvs,
    states,
    decays,
    acc,
    tot,
    raw,
    lifted,
    wide,
    part,
    inbox,
    load_sem,
    x_send,
    x_recv,
    out_send,
    out_recv,
    *sems,
):
    half_width = ALL_WIDTH // 2
    ring = SpGather(
        wall_ref, lambda half: (slice(None), pl.ds(half * half_width, half_width)), sems[:4]
    )
    x = lax.axis_index("tp")
    place = (ring.z, ring.y, ring.c)
    loads = [
        pltpu.make_async_copy(here, there, load_sem.at[k])
        for k, (here, there) in enumerate(
            (
                (wqr_ref, wqr_in),
                (wkr_ref, wkr_in),
                (wvr_ref, wvr_in),
                (wqa_ref, wqa_in),
                (wka_ref, wka_in),
                (wva_ref, wva_in),
                (wor_ref, wor_in),
                (woa_ref, woa_in),
                (tokens_ref, tokens_in),
                (gain_ref, gain_in),
                (cos_ref, cos_in),
                (sin_ref, sin_in),
                (logs_ref, logs_in),
                (gates_ref, gates_in),
            )
        )
    ]
    all_here = greet(*SP_TP)
    for load in loads:
        load.start()
    for load in loads[:-1]:
        load.wait()
    at = 0
    for ref in (wqr_in, wkr_in, wvr_in, wqa_in, wka_in, wva_in, wor_in, woa_in):
        wall_ref[place + (slice(None), slice(at, at + ref.shape[1]))] = ref[...]
        at += ref.shape[1]
    all_here()
    ring.step(0)
    rows = tokens_in[...].astype(jnp.float32)
    x_ref[x] = (
        rows * lax.rsqrt(jnp.mean(rows * rows, axis=-1, keepdims=True) + EPS) * gain_in[...]
    ).astype(jnp.bfloat16)

    def chunk(slot, k):
        return x_ref.at[lax.rem(slot + 4, 4), :, pl.ds(k * 1024, 1024)]

    def pass_on(slot, k, by, sem):
        remote(chunk(slot, k), chunk(slot, k), x_send, x_recv.at[sem], "tp", by).start()

    pass_on(x, 0, 1, 0)
    pass_on(x, 1, -1, 1)
    pass_on(x, 1, 1, 2)
    pass_on(x, 0, -1, 3)
    ring.step(1)
    columns, _ = running_totals(logs_in[...])
    last = columns[SPAN - 1 : SPAN]
    fade = jnp.exp(per_head(last - columns))
    ring.step(2)
    ring.step(3)
    wait_for(chunk(x - 1, 0), x_recv.at[0])
    pass_on(x - 1, 0, 1, 4)
    wait_for(chunk(x + 1, 1), x_recv.at[1])
    pass_on(x + 1, 1, -1, 5)
    for r in range(4, STEPS):
        ring.step(r)
    wait_for(chunk(x - 1, 1), x_recv.at[2])
    wait_for(chunk(x + 1, 0), x_recv.at[3])
    wait_for(chunk(x - 2, 0), x_recv.at[4])
    wait_for(chunk(x + 2, 1), x_recv.at[5])
    ring.finish()
    sent = x_ref.at[pl.ds(0, 3)]
    wait_for(sent, x_send)

    flat = jnp.dot(
        x_ref[...].reshape(SPAN, 2048),
        wall_ref[:, :, :, :, :IN_WIDTH].reshape(2048, IN_WIDTH),
        preferred_element_type=jnp.float32,
    )
    both = flat[:, : 2 * WIDE]
    lane = lax.rem(lax.broadcasted_iota(jnp.int32, both.shape, 1), HEAD)
    turned = jnp.where(
        lane < HEAD // 2, pltpu.roll(both, 2 * WIDE - HEAD // 2, 1), pltpu.roll(both, HEAD // 2, 1)
    )
    cosine = jnp.concatenate([cos_in[...]] * 3, axis=1)
    sine = jnp.concatenate([sin_in[...]] * 3, axis=1)
    roped = both * cosine + turned * sine
    qr_ref[...] = (roped[:, :WIDE] * HEAD**-0.5).astype(jnp.bfloat16)
    key = roped[:, WIDE:].astype(jnp.bfloat16)
    kr_ref[...] = key
    value = flat[:, 2 * WIDE : 3 * WIDE].astype(jnp.bfloat16)
    vr_ref[...] = value
    faded = (key.astype(jnp.float32) * fade).astype(jnp.bfloat16)
    for h in range(3):
        lanes = slice(h * HEAD, (h + 1) * HEAD)
        update[:, lanes] = lax.dot_general(
            faded[:, lanes],
            value[:, lanes],
            (((0,), (0,)), ((), ())),
            preferred_element_type=jnp.float32,
        )
        query = flat[:, 3 * WIDE + h * HEAD : 3 * WIDE + (h + 1) * HEAD] * (HEAD**-0.5 * LOG2E)
        qa_ref[h * SPAN : (h + 1) * SPAN, :] = jnp.concatenate(
            [query, jnp.zeros_like(query)], axis=1
        ).astype(jnp.bfloat16)
    kvs[place] = flat[:, 4 * WIDE :].astype(jnp.bfloat16)


    ring = SpGather(
        kvs, lambda half: (pl.ds(half * (SPAN // 2), SPAN // 2), slice(None)), sems[4:8]
    )
    prefix = Prefix(states, decays, sems[8:])
    mine = ring.z * 16 + ring.y * 2 + ring.c
    prefix.store(ring.c, (update[...], jnp.broadcast_to(per_head(last), (8, WIDE))))
    acc[...] = jnp.zeros_like(acc)
    tot[...] = jnp.zeros_like(tot)
    for s in range(STEPS + 1):
        prefix.step(s)
        if s < STEPS:
            ring.step(s)
        if s == 1:
            retain_inside(qr_ref, kr_ref, vr_ref, logs_in[...], raw, lifted)
    retain_earlier(raw, lifted, prefix.finish().astype(jnp.bfloat16), wide)
    ring.finish()
    loads[-1].wait()

    def gate_row(block, h, blocks):
        span = pl.ds(pl.multiple_of(block * SPAN, SPAN), blocks * SPAN)
        return gates_in[h : h + 1, span] * LOG2E

    gate_columns = jnp.transpose(
        jnp.concatenate(
            [gate_row(mine, h, 1) for h in range(3)] + [jnp.zeros((5, SPAN), jnp.float32)], axis=0
        )
    )

    def weigh(group, masked):
        keys = kvs[group // 2, pl.ds(lax.rem(group, 2) * 4, 4)].reshape(8 * SPAN, 128)
        for h in range(3):
            rows = pl.ds(h * SPAN, SPAN)
            scores = lax.dot_general(
                qa_ref[rows, :], keys, (((1,), (1,)), ((), ())), preferred_element_type=jnp.float32
            )
            logits = scores + (gate_columns[:, h : h + 1] - gate_row(group * 8, h, 8))
            if masked:
                t = lax.broadcasted_iota(jnp.int32, logits.shape, 0)
                s = lax.broadcasted_iota(jnp.int32, logits.shape, 1)
                logits = jnp.where(s - t <= (mine - group * 8) * SPAN, logits, -jnp.inf)
            weights = jnp.exp2(logits)
            total = weights[:, :128]
            for k in range(1, 16):
                total += weights[:, k * 128 : (k + 1) * 128]
            tot[rows, :] += total
            acc[rows, :] += jnp.dot(
                weights.astype(jnp.bfloat16), keys, preferred_element_type=jnp.float32
            )

    def whole(group, carry):
        weigh(group, False)
        return carry

    lax.fori_loop(0, mine // 8, whole, 0)
    weigh(mine // 8, True)
    for h in range(3):
        rows = pl.ds(h * SPAN, SPAN)
        total = jnp.sum(tot[rows, :], axis=1, keepdims=True)
        wide[:, WIDE + h * HEAD : WIDE + (h + 1) * HEAD] = (acc[rows, HEAD:] / total).astype(
            jnp.bfloat16
        )

    def columns(k):
        return pl.ds(k * 512, 512)

    for k in range(4):
        weights = wall_ref[2 * k : 2 * k + 2, :, :, :, IN_WIDTH:].reshape(512, 2 * WIDE)
        part[:, :, k * 512 : (k + 1) * 512] = (
            lax.dot_general(
                wide[...], weights, (((1,), (1,)), ((), ())), preferred_element_type=jnp.float32
            )
            .astype(jnp.bfloat16)
            .reshape(4, SPAN // 4, 512)
        )
        for by in (2, 1, 3):
            remote(
                part.at[lax.rem(x + by, 4), :, columns(k)],
                inbox.at[by - 1, :, columns(k)],
                out_send,
                out_recv.at[by - 1, k],
                "tp",
                by,
            ).start()
    for k in range(4):
        total = part[x, :, k * 512 : (k + 1) * 512].astype(jnp.float32)
        for by in (1, 3, 2):
            wait_for(inbox.at[by - 1, :, columns(k)], out_recv.at[by - 1, k])
            total += inbox[by - 1, :, k * 512 : (k + 1) * 512].astype(jnp.float32)
        out_ref[:, k * 512 : (k + 1) * 512] = total.astype(jnp.bfloat16)
    wait_for(inbox, out_send)


def layer(*operands):
    bf16, f32 = jnp.bfloat16, jnp.float32
    return pl.pallas_call(
        layer_kernel,
        out_shape=jax.ShapeDtypeStruct((SPAN // 4, 2048), bf16),
        in_specs=[ANY] * len(operands),
        out_specs=VMEM,
        scratch_shapes=[
            *(pltpu.VMEM(a.shape, a.dtype) for a in operands),
            pltpu.VMEM((8, 8, 2, 16, ALL_WIDTH), bf16),
            pltpu.VMEM((4, 64, 2048), bf16),
            pltpu.VMEM((SPAN, WIDE), bf16),
            pltpu.VMEM((SPAN, WIDE), bf16),
            pltpu.VMEM((SPAN, WIDE), bf16),
            pltpu.VMEM((3 * SPAN, 128), bf16),
            pltpu.VMEM((HEAD, WIDE), f32),
            pltpu.VMEM((8, 8, 2, SPAN, 128), bf16),
            pltpu.VMEM((18, HEAD, WIDE), bf16),
            pltpu.VMEM((18, 8, WIDE), f32),
            pltpu.VMEM((3 * SPAN, 128), f32),
            pltpu.VMEM((3 * SPAN, 128), f32),
            pltpu.VMEM((SPAN, WIDE), f32),
            pltpu.VMEM((SPAN, WIDE), bf16),
            pltpu.VMEM((SPAN, 2 * WIDE), bf16),
            pltpu.VMEM((4, SPAN // 4, 2048), bf16),
            pltpu.VMEM((3, SPAN // 4, 2048), bf16),
            pltpu.SemaphoreType.DMA((len(operands),)),
            pltpu.SemaphoreType.DMA,
            pltpu.SemaphoreType.DMA((6,)),
            pltpu.SemaphoreType.DMA,
            pltpu.SemaphoreType.DMA((3, 4)),
            *GATHER_SEMS,
            *GATHER_SEMS,
            *PREFIX_SEMS,
        ],
        compiler_params=pltpu.CompilerParams(
            collective_id=1, has_side_effects=True, vmem_limit_bytes=60 * 2**20
        ),
    )(*operands)


def angles_of(positions):
    half = HEAD // 2
    inverse = THETA ** (-jnp.arange(half, dtype=jnp.float32) / half)
    return positions[:, None] * inverse[None, :]


def body(
    tokens,
    pre_gain,
    w_query_ret,
    w_key_ret,
    w_value_ret,
    w_query_att,
    w_key_att,
    w_value_att,
    w_out_ret,
    w_out_att,
    retain_log,
    forget_total,
):
    offset = lax.axis_index(SP) * SPAN
    positions = (offset + jnp.arange(SPAN, dtype=jnp.int32)).astype(jnp.float32)
    angles = angles_of(positions)
    cosine, sine = jnp.cos(angles), jnp.sin(angles)
    cosine = jnp.concatenate([cosine] * 4, axis=1)
    sine = jnp.concatenate([-sine, sine] * 2, axis=1)
    return layer(
        tokens,
        pre_gain.reshape(1, -1),
        w_query_ret,
        w_key_ret,
        w_value_ret,
        w_query_att,
        w_key_att,
        w_value_att,
        w_out_ret.T,
        w_out_att.T,
        cosine,
        sine,
        retain_log.T,
        forget_total,
    )


def solution(mesh):
    finer = Mesh(mesh.devices.reshape(8, 8, 2, mesh.shape["tp"]), ("sp_0", "sp_1", "sp_2", "tp"))
    placed = (
        P(SP_TP, None),
        P(),
        P(SP, "tp"),
        P(SP, "tp"),
        P(SP, "tp"),
        P(SP, "tp"),
        P(SP, "tp"),
        P(SP, "tp"),
        P("tp", SP),
        P("tp", SP),
        P(SP, "tp"),
        P("tp", None),
    )
    return jax.shard_map(
        body, mesh=finer, in_specs=placed, out_specs=P(SP_TP, None), check_vma=False
    )
```

```python
import jax
import jax.numpy as jnp
from jax import lax
from jax.experimental import pallas as pl
from jax.experimental.pallas import tpu as pltpu
from jax.sharding import Mesh
from jax.sharding import PartitionSpec as P

HEAD = 64
SPAN = 256
SP = ("sp_0", "sp_1", "sp_2")
SP_TP = ("sp_0", "sp_1", "sp_2", "tp")
LOG2E = 1.4426950408889634
BY_NAME = pl.DeviceIdType.MESH
VMEM = pl.BlockSpec(memory_space=pltpu.VMEM)
ANY = pl.BlockSpec(memory_space=pl.ANY)
IN_WIDTH = 896
ALL_WIDTH = 1280
WIDE = 3 * HEAD

EPS = 1e-06
THETA = 10000.0

DELTAS = (0, 1, -1, 2, -2, 3, -3, 4)


def ring_plan():
    slots = {}
    for delta in DELTAS[1:]:
        slots["first", delta] = len(slots)
    for delta in DELTAS:
        right = 4 if delta <= 0 else 3
        for way, steps in ((1, right), (-1, 7 - right)):
            for step in range(steps):
                slots[way, delta, step] = len(slots)
    return slots


SLOTS = ring_plan()
STEPS = 9


def greet(*axes):
    barrier = pltpu.get_barrier_semaphore()
    count = 0
    for axis in axes:
        size = lax.axis_size(axis)
        for by in (1, size - 1) if size > 2 else (1,):
            pl.semaphore_signal(
                barrier,
                inc=1,
                device_id={axis: lax.rem(lax.axis_index(axis) + by, size)},
                device_id_type=BY_NAME,
            )
            count += 1
    return lambda: pl.semaphore_wait(barrier, count)


def remote(src, dst, send_sem, recv_sem, axis, by):
    size = lax.axis_size(axis)
    return pltpu.make_async_remote_copy(
        src_ref=src,
        dst_ref=dst,
        send_sem=send_sem,
        recv_sem=recv_sem,
        device_id={axis: lax.rem(lax.axis_index(axis) + by + size, size)},
        device_id_type=BY_NAME,
    )


def wait_for(ref, sem):
    pltpu.make_async_copy(ref, ref, sem).wait()


def ring_index(at):
    return lax.rem(at + 8, 8)


class SpGather:
    def __init__(self, ref, part, sems, by_piece=False):
        self.ref, self.part, self.by_piece = ref, part, by_piece
        self.send_sem, self.recv_sem, self.swap_send, self.swap_recv = sems
        self.z, self.y, self.c = (lax.axis_index(a) for a in SP)

    def piece(self, half, first, second):
        z, y = (second, first) if half == 0 else (first, second)
        return self.ref.at[(z, y, self.c) + self.part(half)]

    def slab(self, half, second):
        place = (second, slice(None)) if half == 0 else (slice(None), second)
        return self.ref.at[place + (self.c,) + self.part(half)]

    def coords(self, half):
        return (self.y, self.z) if half == 0 else (self.z, self.y)

    def send(self, half, ref, axis, by, slot):
        remote(
            ref, ref, self.send_sem.at[half], self.recv_sem.at[half, SLOTS[slot]], axis, by
        ).start()

    def arrived(self, half, ref, slot):
        wait_for(ref, self.recv_sem.at[half, SLOTS[slot]])

    def swap(self, half, second):
        if self.by_piece:
            return
        ref = self.slab(half, second)
        remote(ref, ref, self.swap_send.at[half], self.swap_recv.at[half], "sp_2", 1).start()

    def swap_pieces(self, s):
        for half in (0, 1):
            a, b = self.coords(half)
            for delta in DELTAS:
                for delta_2 in DELTAS:
                    if abs(delta) + abs(delta_2) == s:
                        ref = self.piece(half, ring_index(a - delta), ring_index(b - delta_2))
                        remote(
                            ref,
                            ref,
                            self.swap_send.at[half],
                            self.swap_recv.at[half, s],
                            "sp_2",
                            1,
                        ).start()

    def wait_swapped(self, s):
        rows, columns = ((1, 1), (2, 2), (1, 8), (2, 6), (2, 7), (2, 6), (1, 8), (2, 2), (1, 1))[s]
        for half in (0, 1):
            wait_for(
                self.ref.at[(slice(0, rows), slice(0, columns), 0) + self.part(half)],
                self.swap_recv.at[half, s],
            )

    def step(self, s):
        for half in (0, 1):
            a, b = self.coords(half)
            first, second = ("sp_1", "sp_0") if half == 0 else ("sp_0", "sp_1")
            for delta in sorted({s, -s}, reverse=True):
                if delta not in DELTAS:
                    continue
                ref = self.piece(half, ring_index(a - delta), b)
                if delta:
                    self.arrived(half, ref, ("first", delta))
                for further in (1, -1) if delta == 0 else (delta + (1 if delta > 0 else -1),):
                    if further in DELTAS:
                        self.send(half, ref, first, 1 if further > 0 else -1, ("first", further))
                for by in (1, -1):
                    self.send(half, ref, second, by, (by, delta, 0))
            if s == 4:
                self.swap(half, b)
            for k in range(4):
                for delta in DELTAS:
                    if abs(delta) != s - 1 - k:
                        continue
                    for by in (1, -1):
                        if (by, delta, k) not in SLOTS:
                            continue
                        ref = self.piece(half, ring_index(a - delta), ring_index(b - by * (k + 1)))
                        self.arrived(half, ref, (by, delta, k))
                        if (by, delta, k + 1) in SLOTS:
                            self.send(half, ref, second, by, (by, delta, k + 1))
            if 5 <= s < 8:
                self.swap(half, ring_index(b - (s - 4)))
                self.swap(half, ring_index(b + (s - 4)))
            if s == 8:
                self.swap(half, ring_index(b + 4))

    def finish(self):
        for half in (0, 1):
            core = self.ref.at[(slice(None), slice(None), 0) + self.part(half)]
            if not self.by_piece:
                wait_for(core, self.swap_recv.at[half])
            wait_for(core, self.swap_send.at[half])
            wait_for(
                self.ref.at[(slice(0, 7), slice(None), 0) + self.part(half)],
                self.send_sem.at[half],
            )
            wait_for(
                self.ref.at[(0, slice(0, 7), 0) + self.part(half)], self.send_sem.at[half]
            )


GATHER_SEMS = [
    pltpu.SemaphoreType.DMA((2,)),
    pltpu.SemaphoreType.DMA((2, len(SLOTS))),
    pltpu.SemaphoreType.DMA((2,)),
    pltpu.SemaphoreType.DMA((2,)),
]


def running_totals(logs):
    t = lax.broadcasted_iota(jnp.int32, (SPAN, SPAN), 0)
    s = lax.broadcasted_iota(jnp.int32, (SPAN, SPAN), 1)
    below = jnp.where(s <= t, 1.0, 0.0).astype(jnp.float32)
    dims = (((1,), (1,)), ((), ()))
    exact = lax.Precision.HIGHEST
    columns = lax.dot_general(
        below, logs, dims, preferred_element_type=jnp.float32, precision=exact
    )
    rows = lax.dot_general(logs, below, dims, preferred_element_type=jnp.float32, precision=exact)
    return columns, rows


def per_head(columns):
    rows = columns.shape[0]
    return jnp.concatenate(
        [jnp.broadcast_to(columns[:, h : h + 1], (rows, HEAD)) for h in range(3)], axis=1
    )


class Prefix:
    def __init__(self, states, decays, sems):
        self.states, self.decays = states, decays
        self.state_send, self.state_recv, self.decay_send, self.decay_recv = sems
        self.z, self.y, self.c = (lax.axis_index(a) for a in SP)

    def send(self, slot, axis, by, sem):
        for ref, out, arrive in (
            (self.states, self.state_send, self.state_recv),
            (self.decays, self.decay_send, self.decay_recv),
        ):
            remote(ref.at[slot], ref.at[slot], out, arrive.at[sem], axis, by).start()

    def wait(self, slot, sem):
        wait_for(self.states.at[slot], self.state_recv.at[sem])
        wait_for(self.decays.at[slot], self.decay_recv.at[sem])

    def store(self, slot, pair):
        self.states[slot] = pair[0].astype(jnp.bfloat16)
        self.decays[slot] = pair[1]

    def load(self, slot):
        return self.states[slot].astype(jnp.float32), self.decays[slot]

    @staticmethod
    def join(earlier, later):
        return jnp.exp(later[1][:1]) * earlier[0] + later[0], earlier[1] + later[1]

    @staticmethod
    def keep(flag, pair):
        return jnp.where(flag, pair[0], 0.0), jnp.where(flag, pair[1], 0.0)

    def ring_hop(self, hop, base, here, axis, first_sem):
        if hop == 0:
            self.send(base + here, axis, 1, first_sem)
            self.send(base + here, axis, -1, first_sem + 4)
            return
        right = base + lax.rem(here - hop + 8, 8)
        self.wait(right, first_sem + hop - 1)
        if hop < 4:
            self.send(right, axis, 1, first_sem + hop)
            left = base + lax.rem(here + hop, 8)
            self.wait(left, first_sem + 4 + hop - 1)
            if hop < 3:
                self.send(left, axis, -1, first_sem + 4 + hop)

    def step(self, s):
        if s == 0:
            self.send(self.c, "sp_2", 1, 0)
        if s == 1:
            self.wait(1 - self.c, 0)
            self.store(2 + self.y, self.join(self.load(0), self.load(1)))
            self.ring_hop(0, 2, self.y, "sp_1", 1)
        if 2 <= s <= 5:
            self.ring_hop(s - 1, 2, self.y, "sp_1", 1)
        if s == 5:
            total = self.load(2)
            for k in range(1, 8):
                total = self.join(total, self.load(2 + k))
            self.store(10 + self.z, total)
            self.ring_hop(0, 10, self.z, "sp_0", 8)
        if 6 <= s <= 9:
            self.ring_hop(s - 5, 10, self.z, "sp_0", 8)

    def finish(self):
        before = self.keep(0 < self.z, self.load(10))
        for k in range(1, 7):
            before = self.keep_if(k < self.z, before, self.load(10 + k))
        for k in range(7):
            before = self.keep_if(k < self.y, before, self.load(2 + k))
        before = self.keep_if(self.c == 1, before, self.load(0))
        for ref, sem in ((self.states, self.state_send), (self.decays, self.decay_send)):
            wait_for(ref.at[pl.ds(0, 15)], sem)
        return before[0]

    def keep_if(self, flag, before, later):
        return self.join(before, self.keep(flag, later))


PREFIX_SEMS = [
    pltpu.SemaphoreType.DMA,
    pltpu.SemaphoreType.DMA((15,)),
    pltpu.SemaphoreType.DMA,
    pltpu.SemaphoreType.DMA((15,)),
]


def retain_inside(qr_ref, kr_ref, vr_ref, logs, raw_ref, lifted_ref):
    columns, rows = running_totals(logs)
    t = lax.broadcasted_iota(jnp.int32, (SPAN, SPAN), 0)
    s = lax.broadcasted_iota(jnp.int32, (SPAN, SPAN), 1)
    causal = s <= t
    lifted = qr_ref[...].astype(jnp.float32) * jnp.exp(per_head(columns))
    lifted_ref[...] = lifted.astype(jnp.bfloat16)
    for h in range(3):
        lanes = slice(h * HEAD, (h + 1) * HEAD)
        scores = lax.dot_general(
            qr_ref[:, lanes],
            kr_ref[:, lanes],
            (((1,), (1,)), ((), ())),
            preferred_element_type=jnp.float32,
        )
        gap = jnp.where(causal, columns[:, h : h + 1] - rows[h : h + 1, :], 0.0)
        weights = jnp.where(causal, scores * jnp.exp(gap), 0.0).astype(jnp.bfloat16)
        raw_ref[:, lanes] = jnp.dot(
            weights, vr_ref[:, lanes], preferred_element_type=jnp.float32
        )


def retain_earlier(raw_ref, lifted_ref, before, wide_ref):
    for h in range(3):
        lanes = slice(h * HEAD, (h + 1) * HEAD)
        raw = raw_ref[:, lanes] + jnp.dot(
            lifted_ref[:, lanes], before[:, lanes], preferred_element_type=jnp.float32
        )
        raw -= jnp.mean(raw, axis=-1, keepdims=True)
        spread = jnp.mean(raw * raw, axis=-1, keepdims=True)
        wide_ref[:, lanes] = (raw * lax.rsqrt(spread + EPS)).astype(jnp.bfloat16)


def layer_kernel(
    tokens_ref,
    gain_ref,
    wqr_ref,
    wkr_ref,
    wvr_ref,
    wqa_ref,
    wka_ref,
    wva_ref,
    wor_ref,
    woa_ref,
    cos_ref,
    sin_ref,
    logs_ref,
    gates_ref,
    out_ref,
    tokens_in,
    gain_in,
    wqr_in,
    wkr_in,
    wvr_in,
    wqa_in,
    wka_in,
    wva_in,
    wor_in,
    woa_in,
    cos_in,
    sin_in,
    logs_in,
    gates_in,
    wall_ref,
    x_ref,
    qr_ref,
    kr_ref,
    vr_ref,
    qa_ref,
    update,
    kvs,
    states,
    decays,
    acc,
    tot,
    raw,
    lifted,
    wide,
    part,
    inbox,
    load_sem,
    x_send,
    x_recv,
    out_send,
    out_recv,
    *sems,
):
    half_width = ALL_WIDTH // 2
    ring = SpGather(
        wall_ref, lambda half: (slice(None), pl.ds(half * half_width, half_width)), sems[:4]
    )
    x = lax.axis_index("tp")
    place = (ring.z, ring.y, ring.c)
    loads = [
        pltpu.make_async_copy(here, there, load_sem.at[k])
        for k, (here, there) in enumerate(
            (
                (wqr_ref, wqr_in),
                (wkr_ref, wkr_in),
                (wvr_ref, wvr_in),
                (wqa_ref, wqa_in),
                (wka_ref, wka_in),
                (wva_ref, wva_in),
                (wor_ref, wor_in),
                (woa_ref, woa_in),
                (tokens_ref, tokens_in),
                (gain_ref, gain_in),
                (cos_ref, cos_in),
                (sin_ref, sin_in),
                (logs_ref, logs_in),
                (gates_ref, gates_in),
            )
        )
    ]
    all_here = greet(*SP_TP)
    for load in loads:
        load.start()
    for load in loads[:-1]:
        load.wait()
    at = 0
    for ref in (wqr_in, wkr_in, wvr_in, wqa_in, wka_in, wva_in, wor_in, woa_in):
        wall_ref[place + (slice(None), slice(at, at + ref.shape[1]))] = ref[...]
        at += ref.shape[1]
    all_here()
    ring.step(0)
    rows = tokens_in[...].astype(jnp.float32)
    x_ref[x] = (
        rows * lax.rsqrt(jnp.mean(rows * rows, axis=-1, keepdims=True) + EPS) * gain_in[...]
    ).astype(jnp.bfloat16)

    def chunk(slot, k):
        return x_ref.at[lax.rem(slot + 4, 4), :, pl.ds(k * 1024, 1024)]

    def pass_on(slot, k, by, sem):
        remote(chunk(slot, k), chunk(slot, k), x_send, x_recv.at[sem], "tp", by).start()

    pass_on(x, 0, 1, 0)
    pass_on(x, 1, -1, 1)
    pass_on(x, 1, 1, 2)
    pass_on(x, 0, -1, 3)
    ring.step(1)
    columns, _ = running_totals(logs_in[...])
    last = columns[SPAN - 1 : SPAN]
    fade = jnp.exp(per_head(last - columns))
    ring.step(2)
    ring.step(3)
    wait_for(chunk(x - 1, 0), x_recv.at[0])
    pass_on(x - 1, 0, 1, 4)
    wait_for(chunk(x + 1, 1), x_recv.at[1])
    pass_on(x + 1, 1, -1, 5)
    for r in range(4, STEPS):
        ring.step(r)
    wait_for(chunk(x - 1, 1), x_recv.at[2])
    wait_for(chunk(x + 1, 0), x_recv.at[3])
    wait_for(chunk(x - 2, 0), x_recv.at[4])
    wait_for(chunk(x + 2, 1), x_recv.at[5])
    ring.finish()
    sent = x_ref.at[pl.ds(0, 3)]
    wait_for(sent, x_send)

    flat = jnp.dot(
        x_ref[...].reshape(SPAN, 2048),
        wall_ref[:, :, :, :, :IN_WIDTH].reshape(2048, IN_WIDTH),
        preferred_element_type=jnp.float32,
    )
    both = flat[:, : 2 * WIDE]
    lane = lax.rem(lax.broadcasted_iota(jnp.int32, both.shape, 1), HEAD)
    turned = jnp.where(
        lane < HEAD // 2, pltpu.roll(both, 2 * WIDE - HEAD // 2, 1), pltpu.roll(both, HEAD // 2, 1)
    )
    cosine = jnp.concatenate([cos_in[...]] * 3, axis=1)
    sine = jnp.concatenate([sin_in[...]] * 3, axis=1)
    roped = both * cosine + turned * sine
    qr_ref[...] = (roped[:, :WIDE] * HEAD**-0.5).astype(jnp.bfloat16)
    key = roped[:, WIDE:].astype(jnp.bfloat16)
    kr_ref[...] = key
    value = flat[:, 2 * WIDE : 3 * WIDE].astype(jnp.bfloat16)
    vr_ref[...] = value
    faded = (key.astype(jnp.float32) * fade).astype(jnp.bfloat16)
    for h in range(3):
        lanes = slice(h * HEAD, (h + 1) * HEAD)
        update[:, lanes] = lax.dot_general(
            faded[:, lanes],
            value[:, lanes],
            (((0,), (0,)), ((), ())),
            preferred_element_type=jnp.float32,
        )
        query = flat[:, 3 * WIDE + h * HEAD : 3 * WIDE + (h + 1) * HEAD] * (HEAD**-0.5 * LOG2E)
        qa_ref[h * SPAN : (h + 1) * SPAN, :] = jnp.concatenate(
            [query, jnp.zeros_like(query)], axis=1
        ).astype(jnp.bfloat16)
    kvs[place] = flat[:, 4 * WIDE :].astype(jnp.bfloat16)


    ring = SpGather(
        kvs, lambda half: (pl.ds(half * (SPAN // 2), SPAN // 2), slice(None)), sems[4:8], True
    )
    prefix = Prefix(states, decays, sems[8:])
    mine = ring.z * 16 + ring.y * 2 + ring.c
    prefix.store(ring.c, (update[...], jnp.broadcast_to(per_head(last), (8, WIDE))))
    acc[...] = jnp.zeros_like(acc)
    tot[...] = jnp.zeros_like(tot)
    def gate_row(block, h):
        return gates_in[h : h + 1, pl.ds(pl.multiple_of(block * SPAN, SPAN), SPAN)] * LOG2E

    loads[-1].wait()
    gate_columns = jnp.transpose(
        jnp.concatenate(
            [gate_row(mine, h) for h in range(3)] + [jnp.zeros((5, SPAN), jnp.float32)], axis=0
        )
    )

    def weigh(places, own_first=False):
        blocks = [z * 16 + y * 2 + c for z, y, c in places]
        limits = [mine + (1 if own_first and k == 0 else 0) for k in range(4)]
        allowed = [block < limit for block, limit in zip(blocks, limits)]

        def add():
            keys = jnp.concatenate([kvs[place] for place in places], axis=0)
            for h in range(3):
                rows = pl.ds(h * SPAN, SPAN)
                scores = lax.dot_general(
                    qa_ref[rows, :],
                    keys,
                    (((1,), (1,)), ((), ())),
                    preferred_element_type=jnp.float32,
                )
                fall = jnp.concatenate(
                    [
                        jnp.where(block < limit, gate_row(block, h), jnp.inf)
                        for block, limit in zip(blocks, limits)
                    ],
                    axis=1,
                )
                logits = scores + (gate_columns[:, h : h + 1] - fall)
                if own_first:
                    t = lax.broadcasted_iota(jnp.int32, logits.shape, 0)
                    at = lax.broadcasted_iota(jnp.int32, logits.shape, 1)
                    logits = jnp.where((at >= SPAN) | (at <= t), logits, -jnp.inf)
                weights = jnp.exp2(logits)
                total = weights[:, :128]
                for k in range(1, 8):
                    total += weights[:, k * 128 : (k + 1) * 128]
                tot[rows, :] += total
                acc[rows, :] += jnp.dot(
                    weights.astype(jnp.bfloat16), keys, preferred_element_type=jnp.float32
                )

        if own_first:
            add()
        else:
            pl.when(allowed[0] | allowed[1] | allowed[2] | allowed[3])(add)

    def at_offset(down, across, core):
        return ring_index(ring.z + down), ring_index(ring.y + across), core

    def weigh_distance(distance):
        low, high = max(1, distance - 4), min(3, distance)

        def turns(index, carry):
            q = low + index // 2
            p, core = distance - q, lax.rem(index, 2)
            weigh([at_offset(*off, core) for off in ((p, q), (-q, p), (-p, -q), (q, -p))])
            return carry

        lax.fori_loop(0, 2 * (high - low + 1), turns, 0)

    for s in range(STEPS + 1):
        prefix.step(s)
        if s < STEPS:
            ring.step(s)
            ring.swap_pieces(s)
        if s == 1:
            retain_inside(qr_ref, kr_ref, vr_ref, logs_in[...], raw, lifted)
        if s >= 1:
            ring.wait_swapped(s - 1)
        if 2 <= s <= 8:
            weigh_distance(s - 1)
        if s == 8:
            weigh([at_offset(*off, core) for off in ((0, 4), (4, 0)) for core in (0, 1)])
    weigh(
        [at_offset(*off, core) for off in ((0, 0), (4, 4)) for core in (ring.c, 1 - ring.c)],
        own_first=True,
    )
    retain_earlier(raw, lifted, prefix.finish().astype(jnp.bfloat16), wide)
    ring.finish()
    for h in range(3):
        rows = pl.ds(h * SPAN, SPAN)
        total = jnp.sum(tot[rows, :], axis=1, keepdims=True)
        wide[:, WIDE + h * HEAD : WIDE + (h + 1) * HEAD] = (acc[rows, HEAD:] / total).astype(
            jnp.bfloat16
        )

    def columns(k):
        return pl.ds(k * 512, 512)

    for k in range(4):
        weights = wall_ref[2 * k : 2 * k + 2, :, :, :, IN_WIDTH:].reshape(512, 2 * WIDE)
        part[:, :, k * 512 : (k + 1) * 512] = (
            lax.dot_general(
                wide[...], weights, (((1,), (1,)), ((), ())), preferred_element_type=jnp.float32
            )
            .astype(jnp.bfloat16)
            .reshape(4, SPAN // 4, 512)
        )
        for by in (2, 1, 3):
            remote(
                part.at[lax.rem(x + by, 4), :, columns(k)],
                inbox.at[by - 1, :, columns(k)],
                out_send,
                out_recv.at[by - 1, k],
                "tp",
                by,
            ).start()
    for k in range(4):
        total = part[x, :, k * 512 : (k + 1) * 512].astype(jnp.float32)
        for by in (1, 3, 2):
            wait_for(inbox.at[by - 1, :, columns(k)], out_recv.at[by - 1, k])
            total += inbox[by - 1, :, k * 512 : (k + 1) * 512].astype(jnp.float32)
        out_ref[:, k * 512 : (k + 1) * 512] = total.astype(jnp.bfloat16)
    wait_for(inbox, out_send)


def layer(*operands):
    bf16, f32 = jnp.bfloat16, jnp.float32
    return pl.pallas_call(
        layer_kernel,
        out_shape=jax.ShapeDtypeStruct((SPAN // 4, 2048), bf16),
        in_specs=[ANY] * len(operands),
        out_specs=VMEM,
        scratch_shapes=[
            *(pltpu.VMEM(a.shape, a.dtype) for a in operands),
            pltpu.VMEM((8, 8, 2, 16, ALL_WIDTH), bf16),
            pltpu.VMEM((4, 64, 2048), bf16),
            pltpu.VMEM((SPAN, WIDE), bf16),
            pltpu.VMEM((SPAN, WIDE), bf16),
            pltpu.VMEM((SPAN, WIDE), bf16),
            pltpu.VMEM((3 * SPAN, 128), bf16),
            pltpu.VMEM((HEAD, WIDE), f32),
            pltpu.VMEM((8, 8, 2, SPAN, 128), bf16),
            pltpu.VMEM((18, HEAD, WIDE), bf16),
            pltpu.VMEM((18, 8, WIDE), f32),
            pltpu.VMEM((3 * SPAN, 128), f32),
            pltpu.VMEM((3 * SPAN, 128), f32),
            pltpu.VMEM((SPAN, WIDE), f32),
            pltpu.VMEM((SPAN, WIDE), bf16),
            pltpu.VMEM((SPAN, 2 * WIDE), bf16),
            pltpu.VMEM((4, SPAN // 4, 2048), bf16),
            pltpu.VMEM((3, SPAN // 4, 2048), bf16),
            pltpu.SemaphoreType.DMA((len(operands),)),
            pltpu.SemaphoreType.DMA,
            pltpu.SemaphoreType.DMA((6,)),
            pltpu.SemaphoreType.DMA,
            pltpu.SemaphoreType.DMA((3, 4)),
            *GATHER_SEMS,
            *GATHER_SEMS[:3],
            pltpu.SemaphoreType.DMA((2, STEPS)),
            *PREFIX_SEMS,
        ],
        compiler_params=pltpu.CompilerParams(
            collective_id=1, has_side_effects=True, vmem_limit_bytes=60 * 2**20
        ),
    )(*operands)


def angles_of(positions):
    half = HEAD // 2
    inverse = THETA ** (-jnp.arange(half, dtype=jnp.float32) / half)
    return positions[:, None] * inverse[None, :]


def body(
    tokens,
    pre_gain,
    w_query_ret,
    w_key_ret,
    w_value_ret,
    w_query_att,
    w_key_att,
    w_value_att,
    w_out_ret,
    w_out_att,
    retain_log,
    forget_total,
):
    offset = lax.axis_index(SP) * SPAN
    positions = (offset + jnp.arange(SPAN, dtype=jnp.int32)).astype(jnp.float32)
    angles = angles_of(positions)
    cosine, sine = jnp.cos(angles), jnp.sin(angles)
    cosine = jnp.concatenate([cosine] * 4, axis=1)
    sine = jnp.concatenate([-sine, sine] * 2, axis=1)
    return layer(
        tokens,
        pre_gain.reshape(1, -1),
        w_query_ret,
        w_key_ret,
        w_value_ret,
        w_query_att,
        w_key_att,
        w_value_att,
        w_out_ret.T,
        w_out_att.T,
        cosine,
        sine,
        retain_log.T,
        forget_total,
    )


def solution(mesh):
    finer = Mesh(mesh.devices.reshape(8, 8, 2, mesh.shape["tp"]), ("sp_0", "sp_1", "sp_2", "tp"))
    placed = (
        P(SP_TP, None),
        P(),
        P(SP, "tp"),
        P(SP, "tp"),
        P(SP, "tp"),
        P(SP, "tp"),
        P(SP, "tp"),
        P(SP, "tp"),
        P("tp", SP),
        P("tp", SP),
        P(SP, "tp"),
        P("tp", None),
    )
    return jax.shard_map(
        body, mesh=finer, in_specs=placed, out_specs=P(SP_TP, None), check_vma=False
    )
```

```python
import jax
import jax.numpy as jnp
from jax import lax
from jax.experimental import pallas as pl
from jax.experimental.pallas import tpu as pltpu
from jax.sharding import Mesh
from jax.sharding import PartitionSpec as P

HEAD = 64
SPAN = 256
SP = ("sp_0", "sp_1", "sp_2")
SP_TP = ("sp_0", "sp_1", "sp_2", "tp")
LOG2E = 1.4426950408889634
BY_NAME = pl.DeviceIdType.MESH
VMEM = pl.BlockSpec(memory_space=pltpu.VMEM)
ANY = pl.BlockSpec(memory_space=pl.ANY)
IN_WIDTH = 896
ALL_WIDTH = 1280
WIDE = 3 * HEAD

EPS = 1e-06
THETA = 10000.0

DELTAS = (0, 1, -1, 2, -2, 3, -3, 4)


def ring_plan():
    slots = {}
    for delta in DELTAS[1:]:
        slots["first", delta] = len(slots)
    for delta in DELTAS:
        right = 4 if delta <= 0 else 3
        for way, steps in ((1, right), (-1, 7 - right)):
            for step in range(steps):
                slots[way, delta, step] = len(slots)
    return slots


SLOTS = ring_plan()
STEPS = 9


def greet(*axes):
    barrier = pltpu.get_barrier_semaphore()
    count = 0
    for axis in axes:
        size = lax.axis_size(axis)
        for by in (1, size - 1) if size > 2 else (1,):
            pl.semaphore_signal(
                barrier,
                inc=1,
                device_id={axis: lax.rem(lax.axis_index(axis) + by, size)},
                device_id_type=BY_NAME,
            )
            count += 1
    return lambda: pl.semaphore_wait(barrier, count)


def remote(src, dst, send_sem, recv_sem, axis, by):
    size = lax.axis_size(axis)
    return pltpu.make_async_remote_copy(
        src_ref=src,
        dst_ref=dst,
        send_sem=send_sem,
        recv_sem=recv_sem,
        device_id={axis: lax.rem(lax.axis_index(axis) + by + size, size)},
        device_id_type=BY_NAME,
    )


def wait_for(ref, sem):
    pltpu.make_async_copy(ref, ref, sem).wait()


def ring_index(at):
    return lax.rem(at + 8, 8)


class SpGather:
    def __init__(self, ref, part, sems, by_piece=False):
        self.ref, self.part, self.by_piece = ref, part, by_piece
        self.send_sem, self.recv_sem, self.swap_send, self.swap_recv = sems
        self.z, self.y, self.c = (lax.axis_index(a) for a in SP)

    def piece(self, half, first, second):
        z, y = (second, first) if half == 0 else (first, second)
        return self.ref.at[(z, y, self.c) + self.part(half)]

    def slab(self, half, second):
        place = (second, slice(None)) if half == 0 else (slice(None), second)
        return self.ref.at[place + (self.c,) + self.part(half)]

    def coords(self, half):
        return (self.y, self.z) if half == 0 else (self.z, self.y)

    def send(self, half, ref, axis, by, slot):
        remote(
            ref, ref, self.send_sem.at[half], self.recv_sem.at[half, SLOTS[slot]], axis, by
        ).start()

    def arrived(self, half, ref, slot):
        wait_for(ref, self.recv_sem.at[half, SLOTS[slot]])

    def swap(self, half, second):
        if self.by_piece:
            return
        ref = self.slab(half, second)
        remote(ref, ref, self.swap_send.at[half], self.swap_recv.at[half], "sp_2", 1).start()

    def swap_pieces(self, s):
        for half in (0, 1):
            a, b = self.coords(half)
            for delta in DELTAS:
                for delta_2 in DELTAS:
                    if abs(delta) + abs(delta_2) == s:
                        ref = self.piece(half, ring_index(a - delta), ring_index(b - delta_2))
                        remote(
                            ref,
                            ref,
                            self.swap_send.at[half],
                            self.swap_recv.at[half, s],
                            "sp_2",
                            1,
                        ).start()

    def wait_swapped(self, s):
        rows, columns = ((1, 1), (2, 2), (1, 8), (2, 6), (2, 7), (2, 6), (1, 8), (2, 2), (1, 1))[s]
        for half in (0, 1):
            wait_for(
                self.ref.at[(slice(0, rows), slice(0, columns), 0) + self.part(half)],
                self.swap_recv.at[half, s],
            )

    def step(self, s):
        for delta in sorted({s, -s}, reverse=True):
            if delta in DELTAS:
                for half in (0, 1):
                    self.enter(half, delta)
        for k in range(4):
            for delta in DELTAS:
                if abs(delta) != s - 1 - k:
                    continue
                for by in (1, -1):
                    for half in (0, 1):
                        if (by, delta, k) in SLOTS:
                            self.pass_along(half, by, delta, k)
        for half in (0, 1):
            b = self.coords(half)[1]
            if s == 4:
                self.swap(half, b)
            if 5 <= s < 8:
                self.swap(half, ring_index(b - (s - 4)))
                self.swap(half, ring_index(b + (s - 4)))
            if s == 8:
                self.swap(half, ring_index(b + 4))

    def enter(self, half, delta):
        a, b = self.coords(half)
        first, second = ("sp_1", "sp_0") if half == 0 else ("sp_0", "sp_1")
        ref = self.piece(half, ring_index(a - delta), b)
        if delta:
            self.arrived(half, ref, ("first", delta))
        for further in (1, -1) if delta == 0 else (delta + (1 if delta > 0 else -1),):
            if further in DELTAS:
                self.send(half, ref, first, 1 if further > 0 else -1, ("first", further))
        for by in (1, -1):
            self.send(half, ref, second, by, (by, delta, 0))

    def pass_along(self, half, by, delta, k):
        a, b = self.coords(half)
        ref = self.piece(half, ring_index(a - delta), ring_index(b - by * (k + 1)))
        self.arrived(half, ref, (by, delta, k))
        if (by, delta, k + 1) in SLOTS:
            self.send(half, ref, "sp_0" if half == 0 else "sp_1", by, (by, delta, k + 1))

    def finish(self):
        for half in (0, 1):
            core = self.ref.at[(slice(None), slice(None), 0) + self.part(half)]
            if not self.by_piece:
                wait_for(core, self.swap_recv.at[half])
            wait_for(core, self.swap_send.at[half])
            wait_for(
                self.ref.at[(slice(0, 7), slice(None), 0) + self.part(half)],
                self.send_sem.at[half],
            )
            wait_for(
                self.ref.at[(0, slice(0, 7), 0) + self.part(half)], self.send_sem.at[half]
            )


GATHER_SEMS = [
    pltpu.SemaphoreType.DMA((2,)),
    pltpu.SemaphoreType.DMA((2, len(SLOTS))),
    pltpu.SemaphoreType.DMA((2,)),
    pltpu.SemaphoreType.DMA((2, STEPS)),
]


def running_totals(logs):
    t = lax.broadcasted_iota(jnp.int32, (SPAN, SPAN), 0)
    s = lax.broadcasted_iota(jnp.int32, (SPAN, SPAN), 1)
    below = jnp.where(s <= t, 1.0, 0.0).astype(jnp.float32)
    dims = (((1,), (1,)), ((), ()))
    exact = lax.Precision.HIGHEST
    columns = lax.dot_general(
        below, logs, dims, preferred_element_type=jnp.float32, precision=exact
    )
    rows = lax.dot_general(logs, below, dims, preferred_element_type=jnp.float32, precision=exact)
    return columns, rows


def per_head(columns):
    rows = columns.shape[0]
    return jnp.concatenate(
        [jnp.broadcast_to(columns[:, h : h + 1], (rows, HEAD)) for h in range(3)], axis=1
    )


class Prefix:
    def __init__(self, states, decays, sems):
        self.states, self.decays = states, decays
        self.state_send, self.state_recv, self.decay_send, self.decay_recv = sems
        self.z, self.y, self.c = (lax.axis_index(a) for a in SP)

    def send(self, slot, axis, by, sem):
        for ref, out, arrive in (
            (self.states, self.state_send, self.state_recv),
            (self.decays, self.decay_send, self.decay_recv),
        ):
            remote(ref.at[slot], ref.at[slot], out, arrive.at[sem], axis, by).start()

    def wait(self, slot, sem):
        wait_for(self.states.at[slot], self.state_recv.at[sem])
        wait_for(self.decays.at[slot], self.decay_recv.at[sem])

    def store(self, slot, pair):
        self.states[slot] = pair[0].astype(jnp.bfloat16)
        self.decays[slot] = pair[1]

    def load(self, slot):
        return self.states[slot].astype(jnp.float32), self.decays[slot]

    @staticmethod
    def join(earlier, later):
        return jnp.exp(later[1][:1]) * earlier[0] + later[0], earlier[1] + later[1]

    @staticmethod
    def keep(flag, pair):
        return jnp.where(flag, pair[0], 0.0), jnp.where(flag, pair[1], 0.0)

    def ring_hop(self, hop, base, here, axis, first_sem):
        if hop == 0:
            self.send(base + here, axis, 1, first_sem)
            self.send(base + here, axis, -1, first_sem + 4)
            return
        right = base + lax.rem(here - hop + 8, 8)
        self.wait(right, first_sem + hop - 1)
        if hop < 4:
            self.send(right, axis, 1, first_sem + hop)
            left = base + lax.rem(here + hop, 8)
            self.wait(left, first_sem + 4 + hop - 1)
            if hop < 3:
                self.send(left, axis, -1, first_sem + 4 + hop)

    def step(self, s):
        if s == 0:
            self.send(self.c, "sp_2", 1, 0)
        if s == 1:
            self.wait(1 - self.c, 0)
            self.store(2 + self.y, self.join(self.load(0), self.load(1)))
            self.ring_hop(0, 2, self.y, "sp_1", 1)
        if 2 <= s <= 5:
            self.ring_hop(s - 1, 2, self.y, "sp_1", 1)
        if s == 5:
            total = self.load(2)
            for k in range(1, 8):
                total = self.join(total, self.load(2 + k))
            self.store(10 + self.z, total)
            self.ring_hop(0, 10, self.z, "sp_0", 8)
        if 6 <= s <= 9:
            self.ring_hop(s - 5, 10, self.z, "sp_0", 8)

    def finish(self):
        before = self.keep(0 < self.z, self.load(10))
        for k in range(1, 7):
            before = self.keep_if(k < self.z, before, self.load(10 + k))
        for k in range(7):
            before = self.keep_if(k < self.y, before, self.load(2 + k))
        before = self.keep_if(self.c == 1, before, self.load(0))
        for ref, sem in ((self.states, self.state_send), (self.decays, self.decay_send)):
            wait_for(ref.at[pl.ds(0, 15)], sem)
        return before[0]

    def keep_if(self, flag, before, later):
        return self.join(before, self.keep(flag, later))


PREFIX_SEMS = [
    pltpu.SemaphoreType.DMA,
    pltpu.SemaphoreType.DMA((15,)),
    pltpu.SemaphoreType.DMA,
    pltpu.SemaphoreType.DMA((15,)),
]


def retain_inside(qr_ref, kr_ref, vr_ref, logs, raw_ref, lifted_ref):
    columns, rows = running_totals(logs)
    t = lax.broadcasted_iota(jnp.int32, (SPAN, SPAN), 0)
    s = lax.broadcasted_iota(jnp.int32, (SPAN, SPAN), 1)
    causal = s <= t
    lifted = qr_ref[...].astype(jnp.float32) * jnp.exp(per_head(columns))
    lifted_ref[...] = lifted.astype(jnp.bfloat16)
    for h in range(3):
        lanes = slice(h * HEAD, (h + 1) * HEAD)
        scores = lax.dot_general(
            qr_ref[:, lanes],
            kr_ref[:, lanes],
            (((1,), (1,)), ((), ())),
            preferred_element_type=jnp.float32,
        )
        gap = jnp.where(causal, columns[:, h : h + 1] - rows[h : h + 1, :], 0.0)
        weights = jnp.where(causal, scores * jnp.exp(gap), 0.0).astype(jnp.bfloat16)
        raw_ref[:, lanes] = jnp.dot(
            weights, vr_ref[:, lanes], preferred_element_type=jnp.float32
        )


def retain_earlier(raw_ref, lifted_ref, before, wide_ref):
    for h in range(3):
        lanes = slice(h * HEAD, (h + 1) * HEAD)
        raw = raw_ref[:, lanes] + jnp.dot(
            lifted_ref[:, lanes], before[:, lanes], preferred_element_type=jnp.float32
        )
        raw -= jnp.mean(raw, axis=-1, keepdims=True)
        spread = jnp.mean(raw * raw, axis=-1, keepdims=True)
        wide_ref[:, lanes] = (raw * lax.rsqrt(spread + EPS)).astype(jnp.bfloat16)


def layer_kernel(
    tokens_ref,
    gain_ref,
    wqr_ref,
    wkr_ref,
    wvr_ref,
    wqa_ref,
    wka_ref,
    wva_ref,
    wor_ref,
    woa_ref,
    cos_ref,
    sin_ref,
    logs_ref,
    gates_ref,
    out_ref,
    tokens_in,
    gain_in,
    wqr_in,
    wkr_in,
    wvr_in,
    wqa_in,
    wka_in,
    wva_in,
    wor_in,
    woa_in,
    cos_in,
    sin_in,
    logs_in,
    gates_in,
    wall_ref,
    x_ref,
    qr_ref,
    kr_ref,
    vr_ref,
    qa_ref,
    update,
    kvs,
    states,
    decays,
    acc,
    tot,
    raw,
    lifted,
    wide,
    part,
    inbox,
    load_sem,
    x_send,
    x_recv,
    out_send,
    out_recv,
    *sems,
):
    half_width = ALL_WIDTH // 2
    ring = SpGather(
        wall_ref, lambda half: (slice(None), pl.ds(half * half_width, half_width)), sems[:4], True
    )
    x = lax.axis_index("tp")
    place = (ring.z, ring.y, ring.c)
    loads = [
        pltpu.make_async_copy(here, there, load_sem.at[k])
        for k, (here, there) in enumerate(
            (
                (wqr_ref, wqr_in),
                (wkr_ref, wkr_in),
                (wvr_ref, wvr_in),
                (wqa_ref, wqa_in),
                (wka_ref, wka_in),
                (wva_ref, wva_in),
                (wor_ref, wor_in),
                (woa_ref, woa_in),
                (tokens_ref, tokens_in),
                (gain_ref, gain_in),
                (cos_ref, cos_in),
                (sin_ref, sin_in),
                (logs_ref, logs_in),
                (gates_ref, gates_in),
            )
        )
    ]
    all_here = greet(*SP_TP)
    for load in loads:
        load.start()
    for load in loads[:-1]:
        load.wait()
    at = 0
    for ref in (wqr_in, wkr_in, wvr_in, wqa_in, wka_in, wva_in, wor_in, woa_in):
        wall_ref[place + (slice(None), slice(at, at + ref.shape[1]))] = ref[...]
        at += ref.shape[1]
    all_here()
    ring.step(0)
    rows = tokens_in[...].astype(jnp.float32)
    x_ref[x] = (
        rows * lax.rsqrt(jnp.mean(rows * rows, axis=-1, keepdims=True) + EPS) * gain_in[...]
    ).astype(jnp.bfloat16)

    def chunk(slot, k):
        return x_ref.at[lax.rem(slot + 4, 4), :, pl.ds(k * 1024, 1024)]

    def pass_on(slot, k, by, sem):
        remote(chunk(slot, k), chunk(slot, k), x_send, x_recv.at[sem], "tp", by).start()

    pass_on(x, 0, 1, 0)
    pass_on(x, 1, -1, 1)
    pass_on(x, 1, 1, 2)
    pass_on(x, 0, -1, 3)
    ring.swap_pieces(0)
    ring.step(1)
    ring.swap_pieces(1)
    columns, _ = running_totals(logs_in[...])
    last = columns[SPAN - 1 : SPAN]
    fade = jnp.exp(per_head(last - columns))
    for r in (2, 3):
        ring.step(r)
        ring.swap_pieces(r)
    wait_for(chunk(x - 1, 0), x_recv.at[0])
    pass_on(x - 1, 0, 1, 4)
    wait_for(chunk(x + 1, 1), x_recv.at[1])
    pass_on(x + 1, 1, -1, 5)
    for r in range(4, STEPS):
        ring.step(r)
        ring.swap_pieces(r)
    wait_for(chunk(x - 1, 1), x_recv.at[2])
    wait_for(chunk(x + 1, 0), x_recv.at[3])
    wait_for(chunk(x - 2, 0), x_recv.at[4])
    wait_for(chunk(x + 2, 1), x_recv.at[5])
    for r in range(STEPS):
        ring.wait_swapped(r)
    ring.finish()
    sent = x_ref.at[pl.ds(0, 3)]
    wait_for(sent, x_send)

    flat = jnp.dot(
        x_ref[...].reshape(SPAN, 2048),
        wall_ref[:, :, :, :, :IN_WIDTH].reshape(2048, IN_WIDTH),
        preferred_element_type=jnp.float32,
    )
    both = flat[:, : 2 * WIDE]
    lane = lax.rem(lax.broadcasted_iota(jnp.int32, both.shape, 1), HEAD)
    turned = jnp.where(
        lane < HEAD // 2, pltpu.roll(both, 2 * WIDE - HEAD // 2, 1), pltpu.roll(both, HEAD // 2, 1)
    )
    cosine = jnp.concatenate([cos_in[...]] * 3, axis=1)
    sine = jnp.concatenate([sin_in[...]] * 3, axis=1)
    roped = both * cosine + turned * sine
    qr_ref[...] = (roped[:, :WIDE] * HEAD**-0.5).astype(jnp.bfloat16)
    key = roped[:, WIDE:].astype(jnp.bfloat16)
    kr_ref[...] = key
    value = flat[:, 2 * WIDE : 3 * WIDE].astype(jnp.bfloat16)
    vr_ref[...] = value
    faded = (key.astype(jnp.float32) * fade).astype(jnp.bfloat16)
    for h in range(3):
        lanes = slice(h * HEAD, (h + 1) * HEAD)
        update[:, lanes] = lax.dot_general(
            faded[:, lanes],
            value[:, lanes],
            (((0,), (0,)), ((), ())),
            preferred_element_type=jnp.float32,
        )
        query = flat[:, 3 * WIDE + h * HEAD : 3 * WIDE + (h + 1) * HEAD] * (HEAD**-0.5 * LOG2E)
        qa_ref[h * SPAN : (h + 1) * SPAN, :] = jnp.concatenate(
            [query, jnp.zeros_like(query)], axis=1
        ).astype(jnp.bfloat16)
    kvs[place] = flat[:, 4 * WIDE :].astype(jnp.bfloat16)


    ring = SpGather(
        kvs, lambda half: (pl.ds(half * (SPAN // 2), SPAN // 2), slice(None)), sems[4:8], True
    )
    prefix = Prefix(states, decays, sems[8:])
    mine = ring.z * 16 + ring.y * 2 + ring.c
    prefix.store(ring.c, (update[...], jnp.broadcast_to(per_head(last), (8, WIDE))))
    acc[...] = jnp.zeros_like(acc)
    tot[...] = jnp.zeros_like(tot)
    def gate_row(block, h):
        return gates_in[h : h + 1, pl.ds(pl.multiple_of(block * SPAN, SPAN), SPAN)] * LOG2E

    loads[-1].wait()
    gate_columns = jnp.transpose(
        jnp.concatenate(
            [gate_row(mine, h) for h in range(3)] + [jnp.zeros((5, SPAN), jnp.float32)], axis=0
        )
    )

    def weigh(places, own_first=False):
        blocks = [z * 16 + y * 2 + c for z, y, c in places]
        limits = [mine + (1 if own_first and k == 0 else 0) for k in range(4)]
        allowed = [block < limit for block, limit in zip(blocks, limits)]

        def add():
            keys = jnp.concatenate([kvs[place] for place in places], axis=0)
            for h in range(3):
                rows = pl.ds(h * SPAN, SPAN)
                scores = lax.dot_general(
                    qa_ref[rows, :],
                    keys,
                    (((1,), (1,)), ((), ())),
                    preferred_element_type=jnp.float32,
                )
                fall = jnp.concatenate(
                    [
                        jnp.where(block < limit, gate_row(block, h), jnp.inf)
                        for block, limit in zip(blocks, limits)
                    ],
                    axis=1,
                )
                logits = scores + (gate_columns[:, h : h + 1] - fall)
                if own_first:
                    t = lax.broadcasted_iota(jnp.int32, logits.shape, 0)
                    at = lax.broadcasted_iota(jnp.int32, logits.shape, 1)
                    logits = jnp.where((at >= SPAN) | (at <= t), logits, -jnp.inf)
                weights = jnp.exp2(logits)
                total = weights[:, :128]
                for k in range(1, 8):
                    total += weights[:, k * 128 : (k + 1) * 128]
                tot[rows, :] += total
                acc[rows, :] += jnp.dot(
                    weights.astype(jnp.bfloat16), keys, preferred_element_type=jnp.float32
                )

        if own_first:
            add()
        else:
            pl.when(allowed[0] | allowed[1] | allowed[2] | allowed[3])(add)

    def at_offset(down, across, core):
        return ring_index(ring.z + down), ring_index(ring.y + across), core

    def weigh_distance(distance, core):
        low, high = max(1, distance - 4), min(3, distance)

        def turns(index, carry):
            q = low + index
            p = distance - q
            weigh([at_offset(*off, core) for off in ((p, q), (-q, p), (-p, -q), (q, -p))])
            return carry

        lax.fori_loop(0, high - low + 1, turns, 0)

    for s in range(STEPS + 1):
        prefix.step(s)
        if s < STEPS:
            ring.step(s)
            ring.swap_pieces(s)
        if s == 1:
            retain_inside(qr_ref, kr_ref, vr_ref, logs_in[...], raw, lifted)
        if 1 <= s <= 7:
            weigh_distance(s, ring.c)
        if s >= 1:
            ring.wait_swapped(s - 1)
        if 2 <= s <= 8:
            weigh_distance(s - 1, 1 - ring.c)
        if s == 8:
            weigh([at_offset(*off, core) for off in ((0, 4), (4, 0)) for core in (0, 1)])
    weigh(
        [at_offset(*off, core) for off in ((0, 0), (4, 4)) for core in (ring.c, 1 - ring.c)],
        own_first=True,
    )
    retain_earlier(raw, lifted, prefix.finish().astype(jnp.bfloat16), wide)
    ring.finish()
    for h in range(3):
        rows = pl.ds(h * SPAN, SPAN)
        total = jnp.sum(tot[rows, :], axis=1, keepdims=True)
        wide[:, WIDE + h * HEAD : WIDE + (h + 1) * HEAD] = (acc[rows, HEAD:] / total).astype(
            jnp.bfloat16
        )

    def columns(k):
        return pl.ds(k * 512, 512)

    for k in range(4):
        weights = wall_ref[2 * k : 2 * k + 2, :, :, :, IN_WIDTH:].reshape(512, 2 * WIDE)
        part[:, :, k * 512 : (k + 1) * 512] = (
            lax.dot_general(
                wide[...], weights, (((1,), (1,)), ((), ())), preferred_element_type=jnp.float32
            )
            .astype(jnp.bfloat16)
            .reshape(4, SPAN // 4, 512)
        )
        for by in (2, 1, 3):
            remote(
                part.at[lax.rem(x + by, 4), :, columns(k)],
                inbox.at[by - 1, :, columns(k)],
                out_send,
                out_recv.at[by - 1, k],
                "tp",
                by,
            ).start()
    for k in range(4):
        total = part[x, :, k * 512 : (k + 1) * 512].astype(jnp.float32)
        for by in (1, 3, 2):
            wait_for(inbox.at[by - 1, :, columns(k)], out_recv.at[by - 1, k])
            total += inbox[by - 1, :, k * 512 : (k + 1) * 512].astype(jnp.float32)
        out_ref[:, k * 512 : (k + 1) * 512] = total.astype(jnp.bfloat16)
    wait_for(inbox, out_send)


def layer(*operands):
    bf16, f32 = jnp.bfloat16, jnp.float32
    return pl.pallas_call(
        layer_kernel,
        out_shape=jax.ShapeDtypeStruct((SPAN // 4, 2048), bf16),
        in_specs=[ANY] * len(operands),
        out_specs=VMEM,
        scratch_shapes=[
            *(pltpu.VMEM(a.shape, a.dtype) for a in operands),
            pltpu.VMEM((8, 8, 2, 16, ALL_WIDTH), bf16),
            pltpu.VMEM((4, 64, 2048), bf16),
            pltpu.VMEM((SPAN, WIDE), bf16),
            pltpu.VMEM((SPAN, WIDE), bf16),
            pltpu.VMEM((SPAN, WIDE), bf16),
            pltpu.VMEM((3 * SPAN, 128), bf16),
            pltpu.VMEM((HEAD, WIDE), f32),
            pltpu.VMEM((8, 8, 2, SPAN, 128), bf16),
            pltpu.VMEM((18, HEAD, WIDE), bf16),
            pltpu.VMEM((18, 8, WIDE), f32),
            pltpu.VMEM((3 * SPAN, 128), f32),
            pltpu.VMEM((3 * SPAN, 128), f32),
            pltpu.VMEM((SPAN, WIDE), f32),
            pltpu.VMEM((SPAN, WIDE), bf16),
            pltpu.VMEM((SPAN, 2 * WIDE), bf16),
            pltpu.VMEM((4, SPAN // 4, 2048), bf16),
            pltpu.VMEM((3, SPAN // 4, 2048), bf16),
            pltpu.SemaphoreType.DMA((len(operands),)),
            pltpu.SemaphoreType.DMA,
            pltpu.SemaphoreType.DMA((6,)),
            pltpu.SemaphoreType.DMA,
            pltpu.SemaphoreType.DMA((3, 4)),
            *GATHER_SEMS,
            *GATHER_SEMS,
            *PREFIX_SEMS,
        ],
        compiler_params=pltpu.CompilerParams(
            collective_id=1, has_side_effects=True, vmem_limit_bytes=60 * 2**20
        ),
    )(*operands)


def angles_of(positions):
    half = HEAD // 2
    inverse = THETA ** (-jnp.arange(half, dtype=jnp.float32) / half)
    return positions[:, None] * inverse[None, :]


def body(
    tokens,
    pre_gain,
    w_query_ret,
    w_key_ret,
    w_value_ret,
    w_query_att,
    w_key_att,
    w_value_att,
    w_out_ret,
    w_out_att,
    retain_log,
    forget_total,
):
    offset = lax.axis_index(SP) * SPAN
    positions = (offset + jnp.arange(SPAN, dtype=jnp.int32)).astype(jnp.float32)
    angles = angles_of(positions)
    cosine, sine = jnp.cos(angles), jnp.sin(angles)
    cosine = jnp.concatenate([cosine] * 4, axis=1)
    sine = jnp.concatenate([-sine, sine] * 2, axis=1)
    return layer(
        tokens,
        pre_gain.reshape(1, -1),
        w_query_ret,
        w_key_ret,
        w_value_ret,
        w_query_att,
        w_key_att,
        w_value_att,
        w_out_ret.T,
        w_out_att.T,
        cosine,
        sine,
        retain_log.T,
        forget_total,
    )


def solution(mesh):
    finer = Mesh(mesh.devices.reshape(8, 8, 2, mesh.shape["tp"]), ("sp_0", "sp_1", "sp_2", "tp"))
    placed = (
        P(SP_TP, None),
        P(),
        P(SP, "tp"),
        P(SP, "tp"),
        P(SP, "tp"),
        P(SP, "tp"),
        P(SP, "tp"),
        P(SP, "tp"),
        P("tp", SP),
        P("tp", SP),
        P(SP, "tp"),
        P("tp", None),
    )
    return jax.shard_map(
        body, mesh=finer, in_specs=placed, out_specs=P(SP_TP, None), check_vma=False
    )
```
